32 devices in a mesh: ep: 8 (over z, y), tp: 4 (over x, core).
Axes of the slice: x: 2, y: 2, z: 4, core: 2. Of those that a mesh axis runs over, the one named last changes fastest.
Arguments:
- tokens: bfloat16 [64, 1024], P('ep'), may hold values from -6 to 6
- mix_gain: float32 [1024], replicated, may hold values from 0.1 to 1.9
- w_query: bfloat16 [1024, 512], P(None, 'tp'), may hold values from -0.1875 to 0.1875
- w_key: bfloat16 [1024, 512], P(None, 'tp'), may hold values from -0.1875 to 0.1875
- w_value: bfloat16 [1024, 1024], P(None, 'tp'), may hold values from -0.1875 to 0.1875
- w_ogate: bfloat16 [1024, 1024], P(None, 'tp'), may hold values from -0.1875 to 0.1875
- w_igate: bfloat16 [1024, 4], replicated, may hold values from -0.1875 to 0.1875
- w_fgate: bfloat16 [1024, 4], replicated, may hold values from -0.1875 to 0.1875
- forget_bias: float32 [4], replicated, may hold values from -1 to 3
- head_gain: float32 [1024], P('tp'), may hold values from 0.1 to 1.9
- w_out: bfloat16 [1024, 1024], P('tp'), may hold values from -0.1875 to 0.1875
- memory: float32 [64, 4, 128, 256], P('ep', 'tp'), may hold values from -0.4 to 0.4
- normalizer: float32 [64, 4, 128], P('ep', 'tp'), may hold values from -0.4 to 0.4
- running_max: float32 [64, 4], P('ep', 'tp'), may hold values from -4 to 4
- ffn_gain: float32 [1024], replicated, may hold values from 0.1 to 1.9
- route: int32 [64, 2], replicated, may hold values from 0 to 7, all different within a row; in each aligned block of 64 rows (0 to 63, 64 to 127, ...) at most 32 rows name the same one
- route_weight: float32 [64, 2], replicated, may hold values from 0.05 to 1
- w_gate: bfloat16 [8, 1024, 512], P('ep', None, 'tp'), may hold values from -0.1875 to 0.1875
- w_up: bfloat16 [8, 1024, 512], P('ep', None, 'tp'), may hold values from -0.1875 to 0.1875
- w_down: bfloat16 [8, 512, 1024], P('ep', 'tp'), may hold values from -0.25 to 0.25
Outputs:
- mixed: bfloat16 [64, 1024], P(None, 'ep')
- new_memory: float32 [64, 4, 128, 256], P('ep', 'tp')
- new_normalizer: float32 [64, 4, 128], P('ep', 'tp')
- new_max: float32 [64, 4], P('ep', 'tp')
The draws below stay inside these ranges and needn't reach their ends.
Inputs may be any that keep to these rules, and one draw needn't show every extreme that they name: `route`: each expert is named by at most 32 routes in all, a bound that some block reaches; the two choices of a token differ.
All inputs are finite; a program needn't handle non-finite values.
Results may differ from the reference program's by a relative error of at most 0.014.
Values may be sent and summed in bfloat16 or wider, within the bound.
A program may use at most 64 MiB of HBM per device.

```python
import math
import jax
import jax.numpy as jnp
import numpy as np
from jax import lax

MODEL_WIDTH = 1024
HEADS = 4
QK = 128
DV = 256
EXPERT_HIDDEN = 512
TOPK = 2
TOKENS = 64
EXPERTS = 8
EXPERT_CAPACITY = 32
N_TP = 4


def shard_levels(key, shape, split, low, largest):
    def one(dim, blocks):
        steps = jax.random.uniform(jax.random.fold_in(jax.random.fold_in(key, 6), dim), (blocks,), jnp.float32, low / len(split), largest / len(split))
        return jnp.repeat(jnp.exp(steps), shape[dim] // blocks).reshape((-1,) + (1,) * (len(shape) - dim - 1))

    level = one(*split[0])
    for cut in split[1:]:
        level = level * one(*cut)
    return level


def shared_out(key, own, number, rows, number_of, top, reach, lean):
    ranking = jax.random.permutation(key, number_of)
    packed, common = load_shares(number_of, rows * top, reach, lean, True), load_shares(number_of, rows * top, reach, lean, False)
    places = jnp.arange(number_of)

    def named(sizes, turn):
        used = int((sizes > 0).sum())
        fixed = max(1, used // 4)
        shifted = fixed + (places - fixed + turn * (used - fixed)) % max(1, number_of - fixed)
        return jnp.zeros((number_of,), jnp.int32).at[ranking[jnp.where(places < fixed, places, shifted)]].set(jnp.asarray(sizes, jnp.int32))

    sizes = jnp.where(number % 4 == 0, named(packed, number // 4), named(common, number - number // 4 - 1))
    mixed = jax.random.permutation(jax.random.fold_in(own, 3), number_of)
    source_of, taker = mixed[0:number_of // 2 * 2:2], mixed[1:number_of // 2 * 2:2]
    room = jnp.minimum(sizes[source_of] - 1, reach - sizes[taker]) // 2
    room = jnp.where((source_of == ranking[0]) | (taker == ranking[0]) | (sizes[taker] == 0), 0, jnp.maximum(room, 0))
    shifted = jax.random.randint(jax.random.fold_in(own, 4), (number_of // 2,), 0, 1 << 20) % (room + 1)
    sizes = sizes.at[source_of].add(-shifted).at[taker].add(shifted)
    items = jnp.searchsorted(jnp.cumsum(sizes), jnp.arange(rows * top), side="right").astype(jnp.int32)
    table = items.reshape(top, rows).T
    table = table[jax.random.permutation(jax.random.fold_in(own, 1), rows)]
    turn = jax.random.randint(jax.random.fold_in(own, 2), (rows, 1), 0, top)
    return jnp.take_along_axis(table, (jnp.arange(top)[None, :] + turn) % top, axis=1)


def load_shares(amount, total, most, skew, full):
    portions = [(1 << 20) // math.isqrt(rank ** skew) + 1 for rank in range(1, amount + 1)]
    largest = most if full else min(most, max(-(-total // amount), total * portions[0] // sum(portions)))
    least = 1 if total - largest >= amount - 1 else 0
    holding, spare = [largest] + [least] * (amount - 1), total - largest - least * (amount - 1)
    while spare > 0:
        free = [i for i in range(1, amount) if holding[i] < largest] or [i for i in range(1, amount) if holding[i] < most]
        whole, remaining = sum([portions[i] for i in free]), spare
        for i in free:
            addition = min(most - holding[i], max(1, remaining * portions[i] // whole), spare)
            holding[i] = holding[i] + addition
            spare = spare - addition
    return np.array(holding)


def scatter_about(key, dims, scale, most, split=(), kind=jnp.bfloat16):
    entries = scale * jax.random.normal(key, dims, jnp.float32)
    if split:
        entries = entries * shard_levels(key, dims, split, -0.22, 0.18)
    return jnp.clip(entries, -most, most).astype(kind)


def setup_inputs(seed: int = 0) -> dict:
    arg_keys = jax.random.split(jax.random.key(seed), 21)
    tokens = scatter_about(arg_keys[0], (TOKENS, MODEL_WIDTH), 1.0, 6.0, ((0, 8),))
    mix_gain = jnp.clip(1.0 + 0.18 * jax.random.normal(arg_keys[1], (MODEL_WIDTH,), jnp.float32), 0.1, 1.9)
    w_query = scatter_about(arg_keys[2], (MODEL_WIDTH, HEADS * QK), MODEL_WIDTH ** -0.5, 0.1875, ((1, 4),))
    w_key = scatter_about(arg_keys[3], (MODEL_WIDTH, HEADS * QK), MODEL_WIDTH ** -0.5, 0.1875, ((1, 4),))
    w_value = scatter_about(arg_keys[4], (MODEL_WIDTH, HEADS * DV), MODEL_WIDTH ** -0.5, 0.1875, ((1, 4),))
    w_ogate = scatter_about(arg_keys[5], (MODEL_WIDTH, HEADS * DV), MODEL_WIDTH ** -0.5, 0.1875, ((1, 4),))
    w_igate = scatter_about(arg_keys[6], (MODEL_WIDTH, HEADS), MODEL_WIDTH ** -0.5, 0.1875)
    w_fgate = scatter_about(arg_keys[7], (MODEL_WIDTH, HEADS), MODEL_WIDTH ** -0.5, 0.1875)
    forget_bias = jnp.clip(jax.random.uniform(arg_keys[8], (HEADS,), jnp.float32, -1.0, 3.0), -1.0, 3.0)
    head_gain = jnp.clip(1.0 + 0.18 * jax.random.normal(arg_keys[9], (HEADS * DV,), jnp.float32), 0.1, 1.9)
    w_out = scatter_about(arg_keys[10], (HEADS * DV, MODEL_WIDTH), (HEADS * DV) ** -0.5, 0.1875, ((0, 4),))
    memory = scatter_about(arg_keys[11], (TOKENS, HEADS, QK, DV), 0.06, 0.4, ((0, 8), (1, 4)), jnp.float32)
    normalizer = scatter_about(arg_keys[12], (TOKENS, HEADS, QK), 0.06, 0.4, ((0, 8), (1, 4)), jnp.float32)
    running_max = scatter_about(arg_keys[13], (TOKENS, HEADS), 1.0, 4.0, ((0, 8), (1, 4)), jnp.float32)
    ffn_gain = jnp.clip(1.0 + 0.18 * jax.random.normal(arg_keys[14], (MODEL_WIDTH,), jnp.float32), 0.1, 1.9)
    route_keys = jax.random.split(jax.random.fold_in(arg_keys[15], 1), TOKENS // TOKENS)
    route_turns = jax.random.permutation(jax.random.fold_in(arg_keys[15], 3), TOKENS // TOKENS)
    route = jax.vmap(lambda own, number: shared_out(jax.random.fold_in(arg_keys[15], 2), own, number, TOKENS, EXPERTS, TOPK, EXPERT_CAPACITY, 2))(route_keys, route_turns).reshape((TOKENS, TOPK))
    route_weight = jnp.clip(jnp.exp(jax.random.uniform(arg_keys[16], (TOKENS, TOPK), jnp.float32, math.log(0.05), math.log(1.0))), 0.05, 1.0)
    w_gate = scatter_about(arg_keys[17], (EXPERTS, MODEL_WIDTH, EXPERT_HIDDEN), MODEL_WIDTH ** -0.5, 0.1875, ((0, 8), (2, 4)))
    w_up = scatter_about(arg_keys[18], (EXPERTS, MODEL_WIDTH, EXPERT_HIDDEN), MODEL_WIDTH ** -0.5, 0.1875, ((0, 8), (2, 4)))
    w_down = scatter_about(arg_keys[19], (EXPERTS, EXPERT_HIDDEN, MODEL_WIDTH), EXPERT_HIDDEN ** -0.5, 0.25, ((0, 8), (1, 4)))
    return dict(tokens=tokens, mix_gain=mix_gain, w_query=w_query, w_key=w_key, w_value=w_value, w_ogate=w_ogate, w_igate=w_igate, w_fgate=w_fgate, forget_bias=forget_bias, head_gain=head_gain, w_out=w_out, memory=memory, normalizer=normalizer, running_max=running_max, ffn_gain=ffn_gain, route=route, route_weight=route_weight, w_gate=w_gate, w_up=w_up, w_down=w_down)


EPS = 1e-06

def round_trip(values):
    rounded = lax.optimization_barrier(values.astype(jnp.bfloat16))
    return rounded.astype(jnp.float32)

def norm_rows(values, gain):
    floats = values.astype(jnp.float32)
    scale = lax.rsqrt(lax.optimization_barrier(jnp.mean(floats * floats, axis=-1, keepdims=True)) + EPS)
    return (floats * scale * gain.astype(jnp.float32)).astype(jnp.bfloat16)

def slot_targets(route):
    flat = route.reshape(-1).astype(jnp.int32)
    onehot = (flat[:, None] == jnp.arange(EXPERTS, dtype=jnp.int32)[None, :]).astype(jnp.int32)
    before = jnp.cumsum(onehot, axis=0) - onehot
    slot = lax.optimization_barrier(jnp.sum(before * onehot, axis=1))
    return (flat * EXPERT_CAPACITY + slot).astype(jnp.int32)

def reference(tokens, mix_gain, w_query, w_key, w_value, w_ogate, w_igate, w_fgate, forget_bias, head_gain, w_out, memory, normalizer, running_max, ffn_gain, route, route_weight, w_gate, w_up, w_down):
    count = tokens.shape[0]
    normed = norm_rows(tokens, mix_gain)

    def project(weight, size):
        result = jnp.dot(normed, weight, preferred_element_type=jnp.float32)
        return round_trip(result).reshape(count, HEADS, size)
    query = project(w_query, QK)
    scaled_key = project(w_key, QK) * QK ** (-0.5)
    value = project(w_value, DV)
    ogate = project(w_ogate, DV)
    log_in = jnp.dot(normed, w_igate, preferred_element_type=jnp.float32)
    log_forget = jax.nn.log_sigmoid(jnp.dot(normed, w_fgate, preferred_element_type=jnp.float32) + forget_bias.astype(jnp.float32))
    new_max = jnp.maximum(log_forget + running_max, log_in)
    keep = jnp.exp(log_forget + running_max - new_max)
    admit = jnp.exp(log_in - new_max)
    floor = jnp.exp(-new_max)

    def per_head(items):
        state, norm_state, q_head, k_head, v_head, keep_head, admit_head, floor_head = items
        state = keep_head[:, None, None] * state + admit_head[:, None, None] * k_head[:, :, None] * v_head[:, None, :]
        norm_state = keep_head[:, None] * norm_state + admit_head[:, None] * k_head
        numer = jnp.einsum('tk,tkv->tv', q_head, state, precision=lax.Precision.HIGHEST)
        denom = lax.optimization_barrier(jnp.sum(q_head * norm_state, axis=1))
        read = numer / jnp.maximum(jnp.abs(denom), floor_head)[:, None]
        return (state, norm_state, read)
    heads_first = lambda a: jnp.moveaxis(a, 1, 0)
    states, norms, reads = lax.map(per_head, (heads_first(memory), heads_first(normalizer), heads_first(query), heads_first(scaled_key), heads_first(value), keep.T, admit.T, floor.T))
    new_memory = jnp.moveaxis(states, 0, 1)
    new_normalizer = jnp.moveaxis(norms, 0, 1)
    read = jnp.moveaxis(reads, 0, 1)
    scale = lax.rsqrt(lax.optimization_barrier(jnp.mean(read * read, axis=-1, keepdims=True)) + EPS)
    gated = (jax.nn.sigmoid(ogate) * read * scale * head_gain.reshape(HEADS, DV)).astype(jnp.bfloat16)
    partials = jnp.einsum('thv,hvd->htd', gated.astype(jnp.float32), w_out.reshape(HEADS, DV, MODEL_WIDTH).astype(jnp.float32))
    cell_out = lax.optimization_barrier(jnp.sum(round_trip(partials), axis=0))
    middle = (tokens.astype(jnp.float32) + cell_out).astype(jnp.bfloat16)
    routed_in = norm_rows(middle, ffn_gain)
    targets = slot_targets(route)
    slots = jnp.zeros((EXPERTS * EXPERT_CAPACITY, MODEL_WIDTH), jnp.bfloat16).at[targets].set(jnp.repeat(routed_in, TOPK, axis=0)).reshape(EXPERTS, EXPERT_CAPACITY, MODEL_WIDTH)

    def expert(items):
        rows, gate_m, up_m, down_matrix = items
        gate_v = jnp.dot(rows, gate_m, preferred_element_type=jnp.float32)
        up_v = jnp.dot(rows, up_m, preferred_element_type=jnp.float32)
        activation = (jax.nn.silu(gate_v) * up_v).astype(jnp.bfloat16)
        partial_pieces = jnp.einsum('pxt,xtl->xpl', activation.reshape(EXPERT_CAPACITY, N_TP, EXPERT_HIDDEN // N_TP).astype(jnp.float32), down_matrix.reshape(N_TP, EXPERT_HIDDEN // N_TP, MODEL_WIDTH).astype(jnp.float32))
        return lax.optimization_barrier(jnp.sum(round_trip(partial_pieces), axis=0)).astype(jnp.bfloat16)
    results = lax.map(expert, (slots, w_gate, w_up, w_down))
    picked = results.reshape(EXPERTS * EXPERT_CAPACITY, MODEL_WIDTH)[targets].reshape(count, TOPK, MODEL_WIDTH).astype(jnp.float32)
    weights = route_weight / lax.optimization_barrier(jnp.sum(route_weight, axis=1, keepdims=True))
    mixed = (middle.astype(jnp.float32) + lax.optimization_barrier(jnp.sum(picked * weights[:, :, None], axis=1))).astype(jnp.bfloat16)
    return (mixed, new_memory, new_normalizer, new_max)
```

```python
import functools

import jax
import jax.numpy as jnp
from jax import lax
from jax.experimental import pallas as pl
from jax.experimental.pallas import tpu as pltpu
from jax.sharding import PartitionSpec as P

EXPERT_CAPACITY = 32


EPS = 1e-06


def round_trip(values):
    rounded = lax.optimization_barrier(values.astype(jnp.bfloat16))
    return rounded.astype(jnp.float32)


def norm_rows(values, gain):
    floats = values.astype(jnp.float32)
    scale = lax.rsqrt(jnp.mean(floats * floats, axis=-1, keepdims=True) + EPS)
    return (floats * scale * gain).astype(jnp.bfloat16)


def slot_targets(route, expert_count, capacity):
    flat = route.reshape(-1)
    onehot = (flat[:, None] == jnp.arange(expert_count, dtype=jnp.int32)[None, :]).astype(jnp.int32)
    before = jnp.cumsum(onehot, axis=0) - onehot
    slot = jnp.sum(before * onehot, axis=1)
    return flat * capacity + slot


def shards(
    tokens,
    mix_gain,
    w_query,
    w_key,
    w_value,
    w_ogate,
    w_igate,
    w_fgate,
    forget_bias,
    head_gain,
    w_out,
    memory,
    normalizer,
    running_max,
    ffn_gain,
    route,
    route_weight,
    w_gate,
    w_up,
    w_down,
):
    width = tokens.shape[1]
    col_count = width // lax.axis_size("ep")
    qk_dim = w_query.shape[1]
    normed = norm_rows(tokens, mix_gain)
    query = round_trip(jnp.dot(normed, w_query, preferred_element_type=jnp.float32))
    scaled_key = round_trip(
        jnp.dot(normed, w_key, preferred_element_type=jnp.float32)
    ) * qk_dim ** (-0.5)
    value = round_trip(jnp.dot(normed, w_value, preferred_element_type=jnp.float32))
    ogate = round_trip(jnp.dot(normed, w_ogate, preferred_element_type=jnp.float32))
    head_pick = (jnp.arange(w_igate.shape[1], dtype=jnp.int32) == lax.axis_index("tp")).astype(
        jnp.float32
    )
    log_in = jnp.sum(
        jnp.dot(normed, w_igate, preferred_element_type=jnp.float32) * head_pick, axis=1
    )
    forget_pre = jnp.sum(
        jnp.dot(normed, w_fgate, preferred_element_type=jnp.float32) * head_pick, axis=1
    )
    log_forget = jax.nn.log_sigmoid(forget_pre + jnp.sum(forget_bias * head_pick))
    old_max = running_max[:, 0]
    new_max = jnp.maximum(log_forget + old_max, log_in)
    keep = jnp.exp(log_forget + old_max - new_max)
    admit = jnp.exp(log_in - new_max)
    state = (
        keep[:, None, None] * memory[:, 0]
        + admit[:, None, None] * scaled_key[:, :, None] * value[:, None, :]
    )
    norm_state = keep[:, None] * normalizer[:, 0] + admit[:, None] * scaled_key
    numer = jnp.einsum("tk,tkv->tv", query, state, precision=lax.Precision.HIGHEST)
    denom = jnp.sum(query * norm_state, axis=1)
    read = numer / jnp.maximum(jnp.abs(denom), jnp.exp(-new_max))[:, None]
    scale = lax.rsqrt(jnp.mean(read * read, axis=-1, keepdims=True) + EPS)
    gated = (jax.nn.sigmoid(ogate) * read * scale * head_gain).astype(jnp.bfloat16)
    local_output = lax.psum(
        jnp.dot(gated, w_out, preferred_element_type=jnp.float32).astype(jnp.bfloat16), "tp"
    ).astype(jnp.float32)
    middle_rows = (tokens.astype(jnp.float32) + local_output).astype(jnp.bfloat16)
    middle = lax.all_to_all(middle_rows, "ep", split_axis=1, concat_axis=0, tiled=True)
    expert_count = w_gate.shape[0] * lax.axis_size("ep")
    topk_count = route.shape[1]
    targets = slot_targets(route, expert_count, EXPERT_CAPACITY)
    buffer = (
        jnp.zeros((expert_count * EXPERT_CAPACITY, col_count), jnp.bfloat16)
        .at[targets]
        .set(jnp.repeat(middle, topk_count, axis=0))
    )
    buffer = buffer.reshape(expert_count, EXPERT_CAPACITY, col_count)
    rows = lax.all_to_all(buffer, "ep", split_axis=0, concat_axis=2, tiled=True)
    rows = norm_rows(rows, ffn_gain)
    gate_v = jnp.einsum("ecd,edf->ecf", rows, w_gate, preferred_element_type=jnp.float32)
    up_v = jnp.einsum("ecd,edf->ecf", rows, w_up, preferred_element_type=jnp.float32)
    activation = (jax.nn.silu(gate_v) * up_v).astype(jnp.bfloat16)
    partial_value = jnp.einsum(
        "ecf,efd->ecd", activation, w_down, preferred_element_type=jnp.float32
    )
    results = lax.psum(partial_value.astype(jnp.bfloat16), "tp")
    returned = lax.all_to_all(results, "ep", split_axis=2, concat_axis=0, tiled=True)
    picked = returned.reshape(expert_count * EXPERT_CAPACITY, col_count)[targets]
    picked = picked.reshape(route.shape[0], topk_count, col_count).astype(jnp.float32)
    weights = route_weight / jnp.sum(route_weight, axis=1, keepdims=True)
    mixed = (middle.astype(jnp.float32) + jnp.sum(picked * weights[:, :, None], axis=1)).astype(
        jnp.bfloat16
    )
    return (mixed, state[:, None], norm_state[:, None], new_max[:, None])


MESH = pl.DeviceIdType.MESH


def dot(a, b):
    return jnp.dot(a, b, preferred_element_type=jnp.float32)


def layer_kernel(
    n_ep,
    n_tp,
    cap,
    tokens_ref,
    mix_gain_ref,
    w_query_hbm,
    w_key_hbm,
    w_value_hbm,
    w_ogate_hbm,
    w_igate_ref,
    w_fgate_ref,
    forget_bias_ref,
    head_gain_ref,
    w_out_hbm,
    memory_hbm,
    normalizer_ref,
    running_max_ref,
    ffn_gain_ref,
    route_ref,
    route_weight_ref,
    w_gate_hbm,
    w_up_hbm,
    w_down_hbm,
    mixed_ref,
    new_memory_hbm,
    new_normalizer_ref,
    new_max_ref,
    w_query,
    w_key,
    w_value,
    w_ogate,
    w_out,
    memory,
    w_gate,
    w_up,
    w_down,
    state_buf,
    numer_buf,
    tp_rows,
    ep_rows,
    sent_slots,
    ep_slots,
    tp_mixed,
    load_sem,
    store_sem,
    tp_send,
    tp_recv,
    ep_send,
    ep_recv,
    slot_send,
    slot_recv,
    mix_send,
    mix_recv,
):
    f32, bf16 = jnp.float32, jnp.bfloat16
    ep, tp = lax.axis_index("ep"), lax.axis_index("tp")
    tp_peers = [lax.rem(tp + d, n_tp) for d in range(1, n_tp)]
    ep_peers = [lax.rem(ep + d, n_ep) for d in range(1, n_ep)]

    barrier = pltpu.get_barrier_semaphore()
    for peer in tp_peers:
        pl.semaphore_signal(barrier, inc=1, device_id={"tp": peer}, device_id_type=MESH)
    for peer in ep_peers:
        pl.semaphore_signal(barrier, inc=1, device_id={"ep": peer}, device_id_type=MESH)

    loads = [
        pltpu.make_async_copy(source, target, load_sem.at[i])
        for i, (source, target) in enumerate(
            [
                (w_query_hbm, w_query),
                (w_key_hbm, w_key),
                (w_value_hbm, w_value),
                (w_ogate_hbm, w_ogate),
                (memory_hbm, memory),
                (w_out_hbm, w_out),
                (w_gate_hbm, w_gate),
                (w_up_hbm, w_up),
                (w_down_hbm, w_down),
            ]
        )
    ]
    for load in loads:
        load.start()

    def normalized(floats, gain):
        scale = lax.rsqrt(jnp.mean(floats * floats, axis=-1, keepdims=True) + EPS)
        return (floats * scale * gain).astype(bf16)

    own = tokens_ref.shape[0]
    tokens = tokens_ref[...].astype(f32)
    normed = normalized(tokens, mix_gain_ref[...])
    normed_floats = normed.astype(f32)

    def gate_logit(weight_ref):
        weight = weight_ref[...].astype(f32)
        pick = lax.broadcasted_iota(jnp.int32, weight.shape, 0) == tp
        row = jnp.sum(jnp.where(pick, weight, 0.0), axis=0, keepdims=True)
        return jnp.sum(normed_floats * row, axis=1, keepdims=True)

    log_in = gate_logit(w_igate_ref)
    bias = forget_bias_ref[...]
    bias = jnp.sum(
        jnp.where(lax.broadcasted_iota(jnp.int32, bias.shape, 1) == tp, bias, 0.0),
        axis=1,
        keepdims=True,
    )
    forget_pre = gate_logit(w_fgate_ref) + bias
    log_forget = jnp.minimum(forget_pre, 0.0) - jnp.log1p(jnp.exp(-jnp.abs(forget_pre)))
    eye = lax.broadcasted_iota(jnp.int32, (own, own), 0) == lax.broadcasted_iota(
        jnp.int32, (own, own), 1
    )
    old_max = jnp.sum(jnp.where(eye, running_max_ref[...], 0.0), axis=1, keepdims=True)
    new_max = jnp.maximum(log_forget + old_max, log_in)
    keep = jnp.exp(log_forget + old_max - new_max)
    admit = jnp.exp(log_in - new_max)
    new_max_ref[...] = jnp.sum(jnp.where(eye, new_max, 0.0), axis=0, keepdims=True)

    loads[0].wait()
    query = dot(normed, w_query[...]).astype(bf16).astype(f32)
    loads[1].wait()
    key = dot(normed, w_key[...]).astype(bf16).astype(f32)
    scaled_key = key * w_key.shape[1] ** (-0.5)
    admitted = admit * scaled_key
    loads[2].wait()
    value = dot(normed, w_value[...]).astype(bf16).astype(f32)
    loads[3].wait()
    ogate = dot(normed, w_ogate[...]).astype(bf16).astype(f32)

    norm_state = keep * normalizer_ref[:, 0, :] + admitted
    new_normalizer_ref[:, 0, :] = norm_state
    denom = jnp.sum(query * norm_state, axis=1, keepdims=True)

    query_columns = query.T
    key_columns = admitted.T
    loads[4].wait()
    stores = []
    for t in range(own):
        state = (
            keep[t : t + 1, :] * memory[t]
            + key_columns[:, t : t + 1] * value[t : t + 1, :]
        )
        state_buf[t] = state
        numer_buf[t : t + 1, :] = jnp.sum(
            query_columns[:, t : t + 1] * state, axis=0, keepdims=True
        )
        store = pltpu.make_async_copy(state_buf.at[t], new_memory_hbm.at[t], store_sem.at[t])
        store.start()
        stores.append(store)
    read = numer_buf[...] / jnp.maximum(jnp.abs(denom), jnp.exp(-new_max))
    scale = lax.rsqrt(jnp.mean(read * read, axis=-1, keepdims=True) + EPS)
    gated = (jax.nn.sigmoid(ogate) * read * scale * head_gain_ref[...]).astype(bf16)
    loads[5].wait()
    tp_rows[tp] = dot(gated, w_out[...]).astype(bf16)

    pl.semaphore_wait(barrier, n_tp - 1 + n_ep - 1)

    def exchange(axis, me, peers, source, target, send_sem, recv_sem):
        sends, receipts = [], []
        for peer in peers:
            send = pltpu.make_async_remote_copy(
                src_ref=source(peer),
                dst_ref=target.at[me],
                send_sem=send_sem.at[peer],
                recv_sem=recv_sem.at[me],
                device_id={axis: peer},
                device_id_type=MESH,
            )
            send.start()
            sends.append(send)
            receipts.append(
                pltpu.make_async_remote_copy(
                    src_ref=source(peer),
                    dst_ref=target.at[peer],
                    send_sem=send_sem.at[peer],
                    recv_sem=recv_sem.at[peer],
                    device_id={axis: peer},
                    device_id_type=MESH,
                )
            )
        return sends, receipts

    sends, receipts = exchange(
        "tp", tp, tp_peers, lambda peer: tp_rows.at[tp], tp_rows, tp_send, tp_recv
    )
    all_sends = sends

    count = route_ref.shape[1]
    topk = route_ref.shape[0]
    experts = n_ep
    earlier = (
        lax.broadcasted_iota(jnp.int32, (count, count), 0)
        < lax.broadcasted_iota(jnp.int32, (count, count), 1)
    ).astype(bf16)
    weight_rows = route_weight_ref[...]
    weight_rows = weight_rows / jnp.sum(weight_rows, axis=0, keepdims=True)

    def slot_rows(rows, expert):
        named = route_ref[0:1, :] == expert
        for j in range(1, topk):
            named = named | (route_ref[j : j + 1, :] == expert)
        named = named.astype(f32)
        before = dot(named.astype(bf16), earlier)
        slot = lax.broadcasted_iota(jnp.int32, (rows, count), 0) % cap
        return jnp.where(before == slot.astype(f32), named, 0.0)

    mine = slot_rows(cap, jnp.full((cap, count), ep, jnp.int32))
    chosen_weight = jnp.zeros((1, count), f32)
    for j in range(topk):
        chosen_weight = chosen_weight + jnp.where(
            route_ref[j : j + 1, :] == ep, weight_rows[j : j + 1, :], 0.0
        )
    slot_weight = jnp.sum(mine * chosen_weight, axis=1, keepdims=True)
    mine = mine.astype(bf16)
    every = experts * cap
    combine = slot_rows(
        every, lax.broadcasted_iota(jnp.int32, (every, count), 0) // cap
    ).T.astype(bf16)

    for receipt in receipts:
        receipt.wait_recv()
    summed = tp_rows[0].astype(f32)
    for i in range(1, n_tp):
        summed = summed + tp_rows[i].astype(f32)
    ep_rows[ep] = (tokens + summed).astype(bf16)
    sends, receipts = exchange(
        "ep", ep, ep_peers, lambda peer: ep_rows.at[ep], ep_rows, ep_send, ep_recv
    )
    all_sends = all_sends + sends
    for load in loads[6:]:
        load.wait()
    for receipt in receipts:
        receipt.wait_recv()

    width = tokens.shape[1]
    middle = ep_rows[...].astype(f32).reshape(count, width).astype(bf16)
    rows = normalized(dot(mine, middle), ffn_gain_ref[...])
    gate_v = dot(rows, w_gate[...])
    up_v = dot(rows, w_up[...])
    activation = (gate_v * jax.nn.sigmoid(gate_v) * up_v).astype(bf16)
    partial = (dot(activation, w_down[...]) * slot_weight).astype(bf16)
    columns = width // n_ep
    for c in range(n_ep):
        sent_slots[c] = partial[:, c * columns : (c + 1) * columns]
    sends, receipts = exchange(
        "ep", ep, ep_peers, lambda peer: sent_slots.at[peer], ep_slots, slot_send, slot_recv
    )
    all_sends = all_sends + sends
    ep_slots[ep] = sent_slots[ep]
    own_columns = pl.ds(pl.multiple_of(ep * columns, columns), columns)
    result = ep_rows[:, :, own_columns].astype(f32).reshape(count, columns)
    for receipt in receipts:
        receipt.wait_recv()
    tp_mixed[tp] = dot(combine, ep_slots[...].reshape(every, columns)).astype(bf16)
    sends, receipts = exchange(
        "tp", tp, tp_peers, lambda peer: tp_mixed.at[tp], tp_mixed, mix_send, mix_recv
    )
    all_sends = all_sends + sends
    for store in stores:
        store.wait()
    for receipt in receipts:
        receipt.wait_recv()
    added = tp_mixed[0].astype(f32)
    for i in range(1, n_tp):
        added = added + tp_mixed[i].astype(f32)
    mixed_ref[...] = (result + added).astype(bf16)
    for send in all_sends:
        send.wait_send()


def layer(
    tokens,
    mix_gain,
    w_query,
    w_key,
    w_value,
    w_ogate,
    w_igate,
    w_fgate,
    forget_bias,
    head_gain,
    w_out,
    memory,
    normalizer,
    running_max,
    ffn_gain,
    route,
    route_weight,
    w_gate,
    w_up,
    w_down,
):
    n_ep, n_tp = lax.axis_size("ep"), lax.axis_size("tp")
    own, width = tokens.shape
    columns = width // n_ep
    if columns % 128 or own % 8 or w_gate.shape[0] != 1:
        return shards(
            tokens,
            mix_gain,
            w_query,
            w_key,
            w_value,
            w_ogate,
            w_igate,
            w_fgate,
            forget_bias,
            head_gain,
            w_out,
            memory,
            normalizer,
            running_max,
            ffn_gain,
            route,
            route_weight,
            w_gate,
            w_up,
            w_down,
        )
    cap = EXPERT_CAPACITY
    count = route.shape[0]
    vmem = pl.BlockSpec(memory_space=pltpu.VMEM)
    hbm = pl.BlockSpec(memory_space=pl.ANY)
    bf16, f32 = jnp.bfloat16, jnp.float32
    weights = [w_query, w_key, w_value, w_ogate, w_out, memory[:, 0], w_gate[0], w_up[0], w_down[0]]
    dma = pltpu.SemaphoreType.DMA
    mixed, new_memory, new_normalizer, new_max = pl.pallas_call(
        functools.partial(layer_kernel, n_ep, n_tp, cap),
        out_shape=(
            jax.ShapeDtypeStruct((count, columns), bf16),
            jax.ShapeDtypeStruct(memory[:, 0].shape, f32),
            jax.ShapeDtypeStruct(normalizer.shape, f32),
            jax.ShapeDtypeStruct((1, own), f32),
        ),
        in_specs=[vmem] * 2 + [hbm] * 4 + [vmem] * 4 + [hbm] * 2 + [vmem] * 5 + [hbm] * 3,
        out_specs=(vmem, hbm, vmem, vmem),
        scratch_shapes=[pltpu.VMEM(w.shape, w.dtype) for w in weights]
        + [
            pltpu.VMEM(memory[:, 0].shape, f32),
            pltpu.VMEM((own, w_value.shape[1]), f32),
            pltpu.VMEM((n_tp, own, width), bf16),
            pltpu.VMEM((n_ep, own, width), bf16),
            pltpu.VMEM((n_ep, cap, columns), bf16),
            pltpu.VMEM((n_ep, cap, columns), bf16),
            pltpu.VMEM((n_tp, count, columns), bf16),
            dma((len(weights),)),
            dma((own,)),
            dma((n_tp,)),
            dma((n_tp,)),
            dma((n_ep,)),
            dma((n_ep,)),
            dma((n_ep,)),
            dma((n_ep,)),
            dma((n_tp,)),
            dma((n_tp,)),
        ],
        compiler_params=pltpu.CompilerParams(collective_id=0, has_side_effects=True),
    )(
        tokens,
        mix_gain[None],
        w_query,
        w_key,
        w_value,
        w_ogate,
        w_igate.T,
        w_fgate.T,
        forget_bias[None],
        head_gain[None],
        w_out,
        memory[:, 0],
        normalizer,
        running_max.T,
        ffn_gain[None],
        route.T,
        route_weight.T,
        w_gate[0],
        w_up[0],
        w_down[0],
    )
    return mixed, new_memory[:, None], new_normalizer, new_max.T


def solution(mesh):
    return jax.shard_map(
        layer,
        mesh=mesh,
        in_specs=(
            P("ep", None),
            P(),
            P(None, "tp"),
            P(None, "tp"),
            P(None, "tp"),
            P(None, "tp"),
            P(),
            P(),
            P(),
            P("tp"),
            P("tp", None),
            P("ep", "tp", None, None),
            P("ep", "tp", None),
            P("ep", "tp"),
            P(),
            P(),
            P(),
            P("ep", None, "tp"),
            P("ep", None, "tp"),
            P("ep", "tp", None),
        ),
        out_specs=(P(None, "ep"), P("ep", "tp", None, None), P("ep", "tp", None), P("ep", "tp")),
        check_vma=False,
    )
```

```python
import functools

import jax
import jax.numpy as jnp
from jax import lax
from jax.experimental import pallas as pl
from jax.experimental.pallas import tpu as pltpu
from jax.sharding import PartitionSpec as P

EXPERT_CAPACITY = 32


EPS = 1e-06


def round_trip(values):
    rounded = lax.optimization_barrier(values.astype(jnp.bfloat16))
    return rounded.astype(jnp.float32)


def norm_rows(values, gain):
    floats = values.astype(jnp.float32)
    scale = lax.rsqrt(jnp.mean(floats * floats, axis=-1, keepdims=True) + EPS)
    return (floats * scale * gain).astype(jnp.bfloat16)


def slot_targets(route, expert_count, capacity):
    flat = route.reshape(-1)
    onehot = (flat[:, None] == jnp.arange(expert_count, dtype=jnp.int32)[None, :]).astype(jnp.int32)
    before = jnp.cumsum(onehot, axis=0) - onehot
    slot = jnp.sum(before * onehot, axis=1)
    return flat * capacity + slot


def shards(
    tokens,
    mix_gain,
    w_query,
    w_key,
    w_value,
    w_ogate,
    w_igate,
    w_fgate,
    forget_bias,
    head_gain,
    w_out,
    memory,
    normalizer,
    running_max,
    ffn_gain,
    route,
    route_weight,
    w_gate,
    w_up,
    w_down,
):
    width = tokens.shape[1]
    col_count = width // lax.axis_size("ep")
    qk_dim = w_query.shape[1]
    normed = norm_rows(tokens, mix_gain)
    query = round_trip(jnp.dot(normed, w_query, preferred_element_type=jnp.float32))
    scaled_key = round_trip(
        jnp.dot(normed, w_key, preferred_element_type=jnp.float32)
    ) * qk_dim ** (-0.5)
    value = round_trip(jnp.dot(normed, w_value, preferred_element_type=jnp.float32))
    ogate = round_trip(jnp.dot(normed, w_ogate, preferred_element_type=jnp.float32))
    head_pick = (jnp.arange(w_igate.shape[1], dtype=jnp.int32) == lax.axis_index("tp")).astype(
        jnp.float32
    )
    log_in = jnp.sum(
        jnp.dot(normed, w_igate, preferred_element_type=jnp.float32) * head_pick, axis=1
    )
    forget_pre = jnp.sum(
        jnp.dot(normed, w_fgate, preferred_element_type=jnp.float32) * head_pick, axis=1
    )
    log_forget = jax.nn.log_sigmoid(forget_pre + jnp.sum(forget_bias * head_pick))
    old_max = running_max[:, 0]
    new_max = jnp.maximum(log_forget + old_max, log_in)
    keep = jnp.exp(log_forget + old_max - new_max)
    admit = jnp.exp(log_in - new_max)
    state = (
        keep[:, None, None] * memory[:, 0]
        + admit[:, None, None] * scaled_key[:, :, None] * value[:, None, :]
    )
    norm_state = keep[:, None] * normalizer[:, 0] + admit[:, None] * scaled_key
    numer = jnp.einsum("tk,tkv->tv", query, state, precision=lax.Precision.HIGHEST)
    denom = jnp.sum(query * norm_state, axis=1)
    read = numer / jnp.maximum(jnp.abs(denom), jnp.exp(-new_max))[:, None]
    scale = lax.rsqrt(jnp.mean(read * read, axis=-1, keepdims=True) + EPS)
    gated = (jax.nn.sigmoid(ogate) * read * scale * head_gain).astype(jnp.bfloat16)
    local_output = lax.psum(
        jnp.dot(gated, w_out, preferred_element_type=jnp.float32).astype(jnp.bfloat16), "tp"
    ).astype(jnp.float32)
    middle_rows = (tokens.astype(jnp.float32) + local_output).astype(jnp.bfloat16)
    middle = lax.all_to_all(middle_rows, "ep", split_axis=1, concat_axis=0, tiled=True)
    expert_count = w_gate.shape[0] * lax.axis_size("ep")
    topk_count = route.shape[1]
    targets = slot_targets(route, expert_count, EXPERT_CAPACITY)
    buffer = (
        jnp.zeros((expert_count * EXPERT_CAPACITY, col_count), jnp.bfloat16)
        .at[targets]
        .set(jnp.repeat(middle, topk_count, axis=0))
    )
    buffer = buffer.reshape(expert_count, EXPERT_CAPACITY, col_count)
    rows = lax.all_to_all(buffer, "ep", split_axis=0, concat_axis=2, tiled=True)
    rows = norm_rows(rows, ffn_gain)
    gate_v = jnp.einsum("ecd,edf->ecf", rows, w_gate, preferred_element_type=jnp.float32)
    up_v = jnp.einsum("ecd,edf->ecf", rows, w_up, preferred_element_type=jnp.float32)
    activation = (jax.nn.silu(gate_v) * up_v).astype(jnp.bfloat16)
    partial_value = jnp.einsum(
        "ecf,efd->ecd", activation, w_down, preferred_element_type=jnp.float32
    )
    results = lax.psum(partial_value.astype(jnp.bfloat16), "tp")
    returned = lax.all_to_all(results, "ep", split_axis=2, concat_axis=0, tiled=True)
    picked = returned.reshape(expert_count * EXPERT_CAPACITY, col_count)[targets]
    picked = picked.reshape(route.shape[0], topk_count, col_count).astype(jnp.float32)
    weights = route_weight / jnp.sum(route_weight, axis=1, keepdims=True)
    mixed = (middle.astype(jnp.float32) + jnp.sum(picked * weights[:, :, None], axis=1)).astype(
        jnp.bfloat16
    )
    return (mixed, state[:, None], norm_state[:, None], new_max[:, None])


MESH = pl.DeviceIdType.MESH


def dot(a, b):
    return jnp.dot(a, b, preferred_element_type=jnp.float32)


LOAD_ORDER = (
    0,
    1,
    6,
    7,
    8,
    13,
    2,
    3,
    4,
    5,
    12,
    11,
    9,
    10,
    15,
    16,
    14,
    17,
    18,
    19,
)


def layer_kernel(n_ep, n_tp, cap, *refs):
    arguments, refs = refs[: len(LOAD_ORDER)], refs[len(LOAD_ORDER) :]
    (mixed_ref, state_buf, new_normalizer_ref, new_max_ref), refs = refs[:4], refs[4:]
    staged, refs = refs[: len(LOAD_ORDER)], refs[len(LOAD_ORDER) :]
    (
        tokens_ref,
        mix_gain_ref,
        w_query,
        w_key,
        w_value,
        w_ogate,
        w_igate_ref,
        w_fgate_ref,
        forget_bias_ref,
        head_gain_ref,
        w_out,
        memory,
        normalizer_ref,
        running_max_ref,
        ffn_gain_ref,
        route_ref,
        route_weight_ref,
        w_gate,
        w_up,
        w_down,
    ) = staged
    (
        numer_buf,
        tp_rows,
        ep_rows,
        sent_slots,
        ep_slots,
        tp_mixed,
        load_sem,
        tp_send,
        tp_recv,
        ep_send,
        ep_recv,
        slot_send,
        slot_recv,
        mix_send,
        mix_recv,
    ) = refs
    f32, bf16 = jnp.float32, jnp.bfloat16
    ep, tp = lax.axis_index("ep"), lax.axis_index("tp")
    tp_peers = [lax.rem(tp + d, n_tp) for d in range(1, n_tp)]
    ep_peers = [lax.rem(ep + d, n_ep) for d in range(1, n_ep)]

    barrier = pltpu.get_barrier_semaphore()
    for peer in tp_peers:
        pl.semaphore_signal(barrier, inc=1, device_id={"tp": peer}, device_id_type=MESH)
    for peer in ep_peers:
        pl.semaphore_signal(barrier, inc=1, device_id={"ep": peer}, device_id_type=MESH)

    loads = {}
    for i in LOAD_ORDER:
        loads[i] = pltpu.make_async_copy(arguments[i], staged[i], load_sem.at[i])
        loads[i].start()

    def arrived(*which):
        for ref in which:
            for i, target in enumerate(staged):
                if target is ref:
                    loads[i].wait()

    def normalized(floats, gain):
        scale = lax.rsqrt(jnp.mean(floats * floats, axis=-1, keepdims=True) + EPS)
        return (floats * scale * gain).astype(bf16)

    own = tokens_ref.shape[0]
    arrived(tokens_ref, mix_gain_ref)
    tokens = tokens_ref[...].astype(f32)
    normed = normalized(tokens, mix_gain_ref[...])
    normed_floats = normed.astype(f32)

    def gate_logit(weight_ref):
        weight = weight_ref[...].astype(f32)
        pick = lax.broadcasted_iota(jnp.int32, weight.shape, 0) == tp
        row = jnp.sum(jnp.where(pick, weight, 0.0), axis=0, keepdims=True)
        return jnp.sum(normed_floats * row, axis=1, keepdims=True)

    arrived(w_igate_ref, w_fgate_ref, forget_bias_ref, running_max_ref)
    log_in = gate_logit(w_igate_ref)
    bias = forget_bias_ref[...]
    bias = jnp.sum(
        jnp.where(lax.broadcasted_iota(jnp.int32, bias.shape, 1) == tp, bias, 0.0),
        axis=1,
        keepdims=True,
    )
    forget_pre = gate_logit(w_fgate_ref) + bias
    log_forget = jnp.minimum(forget_pre, 0.0) - jnp.log1p(jnp.exp(-jnp.abs(forget_pre)))
    eye = lax.broadcasted_iota(jnp.int32, (own, own), 0) == lax.broadcasted_iota(
        jnp.int32, (own, own), 1
    )
    old_max = jnp.sum(jnp.where(eye, running_max_ref[...], 0.0), axis=1, keepdims=True)
    new_max = jnp.maximum(log_forget + old_max, log_in)
    keep = jnp.exp(log_forget + old_max - new_max)
    admit = jnp.exp(log_in - new_max)
    new_max_ref[...] = jnp.sum(jnp.where(eye, new_max, 0.0), axis=0, keepdims=True)

    arrived(w_query)
    query = dot(normed, w_query[...]).astype(bf16).astype(f32)
    arrived(w_key)
    key = dot(normed, w_key[...]).astype(bf16).astype(f32)
    scaled_key = key * w_key.shape[1] ** (-0.5)
    admitted = admit * scaled_key
    arrived(w_value)
    value = dot(normed, w_value[...]).astype(bf16).astype(f32)
    arrived(w_ogate, normalizer_ref)
    ogate = dot(normed, w_ogate[...]).astype(bf16).astype(f32)

    norm_state = keep * normalizer_ref[:, 0, :] + admitted
    new_normalizer_ref[:, 0, :] = norm_state
    denom = jnp.sum(query * norm_state, axis=1, keepdims=True)

    query_columns = query.T
    key_columns = admitted.T
    arrived(memory)
    for t in range(own):
        state = (
            keep[t : t + 1, :] * memory[t]
            + key_columns[:, t : t + 1] * value[t : t + 1, :]
        )
        state_buf[t] = state
        numer_buf[t : t + 1, :] = jnp.sum(
            query_columns[:, t : t + 1] * state, axis=0, keepdims=True
        )
    arrived(head_gain_ref)
    read = numer_buf[...] / jnp.maximum(jnp.abs(denom), jnp.exp(-new_max))
    scale = lax.rsqrt(jnp.mean(read * read, axis=-1, keepdims=True) + EPS)
    gated = (jax.nn.sigmoid(ogate) * read * scale * head_gain_ref[...]).astype(bf16)
    arrived(w_out)
    tp_rows[tp] = dot(gated, w_out[...]).astype(bf16)

    pl.semaphore_wait(barrier, n_tp - 1 + n_ep - 1)

    def exchange(axis, me, peers, source, target, send_sem, recv_sem):
        sends, receipts = [], []
        for peer in peers:
            send = pltpu.make_async_remote_copy(
                src_ref=source(peer),
                dst_ref=target.at[me],
                send_sem=send_sem.at[peer],
                recv_sem=recv_sem.at[me],
                device_id={axis: peer},
                device_id_type=MESH,
            )
            send.start()
            sends.append(send)
            receipts.append(
                pltpu.make_async_remote_copy(
                    src_ref=source(peer),
                    dst_ref=target.at[peer],
                    send_sem=send_sem.at[peer],
                    recv_sem=recv_sem.at[peer],
                    device_id={axis: peer},
                    device_id_type=MESH,
                )
            )
        return sends, receipts

    sends, receipts = exchange(
        "tp", tp, tp_peers, lambda peer: tp_rows.at[tp], tp_rows, tp_send, tp_recv
    )
    all_sends = sends

    arrived(route_ref, route_weight_ref)
    count = route_ref.shape[1]
    topk = route_ref.shape[0]
    experts = n_ep
    earlier = (
        lax.broadcasted_iota(jnp.int32, (count, count), 0)
        < lax.broadcasted_iota(jnp.int32, (count, count), 1)
    ).astype(bf16)
    weight_rows = route_weight_ref[...]
    weight_rows = weight_rows / jnp.sum(weight_rows, axis=0, keepdims=True)

    def slot_rows(rows, expert):
        named = route_ref[0:1, :] == expert
        for j in range(1, topk):
            named = named | (route_ref[j : j + 1, :] == expert)
        named = named.astype(f32)
        before = dot(named.astype(bf16), earlier)
        slot = lax.broadcasted_iota(jnp.int32, (rows, count), 0) % cap
        return jnp.where(before == slot.astype(f32), named, 0.0)

    mine = slot_rows(cap, jnp.full((cap, count), ep, jnp.int32))
    chosen_weight = jnp.zeros((1, count), f32)
    for j in range(topk):
        chosen_weight = chosen_weight + jnp.where(
            route_ref[j : j + 1, :] == ep, weight_rows[j : j + 1, :], 0.0
        )
    slot_weight = jnp.sum(mine * chosen_weight, axis=1, keepdims=True)
    mine = mine.astype(bf16)
    every = experts * cap
    combine = slot_rows(
        every, lax.broadcasted_iota(jnp.int32, (every, count), 0) // cap
    ).T.astype(bf16)

    for receipt in receipts:
        receipt.wait_recv()
    summed = tp_rows[0].astype(f32)
    for i in range(1, n_tp):
        summed = summed + tp_rows[i].astype(f32)
    ep_rows[ep] = (tokens + summed).astype(bf16)
    sends, receipts = exchange(
        "ep", ep, ep_peers, lambda peer: ep_rows.at[ep], ep_rows, ep_send, ep_recv
    )
    all_sends = all_sends + sends
    arrived(ffn_gain_ref, w_gate, w_up, w_down)
    for receipt in receipts:
        receipt.wait_recv()

    width = tokens.shape[1]
    middle = ep_rows[...].astype(f32).reshape(count, width).astype(bf16)
    rows = normalized(dot(mine, middle), ffn_gain_ref[...])
    gate_v = dot(rows, w_gate[...])
    up_v = dot(rows, w_up[...])
    activation = (gate_v * jax.nn.sigmoid(gate_v) * up_v).astype(bf16)
    partial = (dot(activation, w_down[...]) * slot_weight).astype(bf16)
    columns = width // n_ep
    for c in range(n_ep):
        sent_slots[c] = partial[:, c * columns : (c + 1) * columns]
    sends, receipts = exchange(
        "ep", ep, ep_peers, lambda peer: sent_slots.at[peer], ep_slots, slot_send, slot_recv
    )
    all_sends = all_sends + sends
    ep_slots[ep] = sent_slots[ep]
    own_columns = pl.ds(pl.multiple_of(ep * columns, columns), columns)
    result = ep_rows[:, :, own_columns].astype(f32).reshape(count, columns)
    for receipt in receipts:
        receipt.wait_recv()
    tp_mixed[tp] = dot(combine, ep_slots[...].reshape(every, columns)).astype(bf16)
    sends, receipts = exchange(
        "tp", tp, tp_peers, lambda peer: tp_mixed.at[tp], tp_mixed, mix_send, mix_recv
    )
    all_sends = all_sends + sends
    for receipt in receipts:
        receipt.wait_recv()
    added = tp_mixed[0].astype(f32)
    for i in range(1, n_tp):
        added = added + tp_mixed[i].astype(f32)
    mixed_ref[...] = (result + added).astype(bf16)
    for send in all_sends:
        send.wait_send()


def write_results(*refs):
    sem = refs[-1]
    half = (len(refs) - 1) // 2
    copies = [
        pltpu.make_async_copy(source, target, sem.at[i])
        for i, (source, target) in enumerate(zip(refs[:half], refs[half:-1]))
    ]
    for copy in copies:
        copy.start()
    for copy in copies:
        copy.wait()


def layer(
    tokens,
    mix_gain,
    w_query,
    w_key,
    w_value,
    w_ogate,
    w_igate,
    w_fgate,
    forget_bias,
    head_gain,
    w_out,
    memory,
    normalizer,
    running_max,
    ffn_gain,
    route,
    route_weight,
    w_gate,
    w_up,
    w_down,
):
    n_ep, n_tp = lax.axis_size("ep"), lax.axis_size("tp")
    own, width = tokens.shape
    columns = width // n_ep
    if columns % 128 or own % 8 or w_gate.shape[0] != 1:
        return shards(
            tokens,
            mix_gain,
            w_query,
            w_key,
            w_value,
            w_ogate,
            w_igate,
            w_fgate,
            forget_bias,
            head_gain,
            w_out,
            memory,
            normalizer,
            running_max,
            ffn_gain,
            route,
            route_weight,
            w_gate,
            w_up,
            w_down,
        )
    cap = EXPERT_CAPACITY
    count = route.shape[0]
    anywhere = pl.BlockSpec(memory_space=pltpu.HBM)
    vmem = pl.BlockSpec(memory_space=pltpu.VMEM)
    bf16, f32 = jnp.bfloat16, jnp.float32
    operands = [
        tokens,
        mix_gain[None],
        w_query,
        w_key,
        w_value,
        w_ogate,
        w_igate.T,
        w_fgate.T,
        forget_bias[None],
        head_gain[None],
        w_out,
        memory[:, 0],
        normalizer,
        running_max.T,
        ffn_gain[None],
        route.T,
        route_weight.T,
        w_gate[0],
        w_up[0],
        w_down[0],
    ]
    dma = pltpu.SemaphoreType.DMA
    results = [
        ((count, columns), bf16),
        (memory[:, 0].shape, f32),
        (normalizer.shape, f32),
        ((1, own), f32),
    ]
    held = pl.pallas_call(
        functools.partial(layer_kernel, n_ep, n_tp, cap),
        out_shape=tuple(pltpu.VMEM(*result) for result in results),
        in_specs=[anywhere] * len(operands),
        out_specs=(vmem,) * len(results),
        scratch_shapes=[pltpu.VMEM(a.shape, a.dtype) for a in operands]
        + [
            pltpu.VMEM((own, w_value.shape[1]), f32),
            pltpu.VMEM((n_tp, own, width), bf16),
            pltpu.VMEM((n_ep, own, width), bf16),
            pltpu.VMEM((n_ep, cap, columns), bf16),
            pltpu.VMEM((n_ep, cap, columns), bf16),
            pltpu.VMEM((n_tp, count, columns), bf16),
            dma((len(operands),)),
            dma((n_tp,)),
            dma((n_tp,)),
            dma((n_ep,)),
            dma((n_ep,)),
            dma((n_ep,)),
            dma((n_ep,)),
            dma((n_tp,)),
            dma((n_tp,)),
        ],
        compiler_params=pltpu.CompilerParams(
            collective_id=0, has_side_effects=True
        ),
    )(*operands)
    mixed, new_memory, new_normalizer, new_max = pl.pallas_call(
        write_results,
        out_shape=tuple(jax.ShapeDtypeStruct(*result) for result in results),
        in_specs=[vmem] * len(results),
        out_specs=(anywhere,) * len(results),
        scratch_shapes=[dma((len(results),))],
        compiler_params=pltpu.CompilerParams(vmem_limit_bytes=1024 * 1024),
    )(*held)
    return mixed, new_memory[:, None], new_normalizer, new_max.T


def solution(mesh):
    return jax.shard_map(
        layer,
        mesh=mesh,
        in_specs=(
            P("ep", None),
            P(),
            P(None, "tp"),
            P(None, "tp"),
            P(None, "tp"),
            P(None, "tp"),
            P(),
            P(),
            P(),
            P("tp"),
            P("tp", None),
            P("ep", "tp", None, None),
            P("ep", "tp", None),
            P("ep", "tp"),
            P(),
            P(),
            P(),
            P("ep", None, "tp"),
            P("ep", None, "tp"),
            P("ep", "tp", None),
        ),
        out_specs=(P(None, "ep"), P("ep", "tp", None, None), P("ep", "tp", None), P("ep", "tp")),
        check_vma=False,
    )
```

```python
import functools

import jax
import jax.numpy as jnp
from jax import lax
from jax.experimental import pallas as pl
from jax.experimental.pallas import tpu as pltpu
from jax.sharding import PartitionSpec as P

EXPERT_CAPACITY = 32


EPS = 1e-06


def round_trip(values):
    rounded = lax.optimization_barrier(values.astype(jnp.bfloat16))
    return rounded.astype(jnp.float32)


def norm_rows(values, gain):
    floats = values.astype(jnp.float32)
    scale = lax.rsqrt(jnp.mean(floats * floats, axis=-1, keepdims=True) + EPS)
    return (floats * scale * gain).astype(jnp.bfloat16)


def slot_targets(route, expert_count, capacity):
    flat = route.reshape(-1)
    onehot = (flat[:, None] == jnp.arange(expert_count, dtype=jnp.int32)[None, :]).astype(jnp.int32)
    before = jnp.cumsum(onehot, axis=0) - onehot
    slot = jnp.sum(before * onehot, axis=1)
    return flat * capacity + slot


def shards(
    tokens,
    mix_gain,
    w_query,
    w_key,
    w_value,
    w_ogate,
    w_igate,
    w_fgate,
    forget_bias,
    head_gain,
    w_out,
    memory,
    normalizer,
    running_max,
    ffn_gain,
    route,
    route_weight,
    w_gate,
    w_up,
    w_down,
):
    width = tokens.shape[1]
    col_count = width // lax.axis_size("ep")
    qk_dim = w_query.shape[1]
    normed = norm_rows(tokens, mix_gain)
    query = round_trip(jnp.dot(normed, w_query, preferred_element_type=jnp.float32))
    scaled_key = round_trip(
        jnp.dot(normed, w_key, preferred_element_type=jnp.float32)
    ) * qk_dim ** (-0.5)
    value = round_trip(jnp.dot(normed, w_value, preferred_element_type=jnp.float32))
    ogate = round_trip(jnp.dot(normed, w_ogate, preferred_element_type=jnp.float32))
    head_pick = (jnp.arange(w_igate.shape[1], dtype=jnp.int32) == lax.axis_index("tp")).astype(
        jnp.float32
    )
    log_in = jnp.sum(
        jnp.dot(normed, w_igate, preferred_element_type=jnp.float32) * head_pick, axis=1
    )
    forget_pre = jnp.sum(
        jnp.dot(normed, w_fgate, preferred_element_type=jnp.float32) * head_pick, axis=1
    )
    log_forget = jax.nn.log_sigmoid(forget_pre + jnp.sum(forget_bias * head_pick))
    old_max = running_max[:, 0]
    new_max = jnp.maximum(log_forget + old_max, log_in)
    keep = jnp.exp(log_forget + old_max - new_max)
    admit = jnp.exp(log_in - new_max)
    state = (
        keep[:, None, None] * memory[:, 0]
        + admit[:, None, None] * scaled_key[:, :, None] * value[:, None, :]
    )
    norm_state = keep[:, None] * normalizer[:, 0] + admit[:, None] * scaled_key
    numer = jnp.einsum("tk,tkv->tv", query, state, precision=lax.Precision.HIGHEST)
    denom = jnp.sum(query * norm_state, axis=1)
    read = numer / jnp.maximum(jnp.abs(denom), jnp.exp(-new_max))[:, None]
    scale = lax.rsqrt(jnp.mean(read * read, axis=-1, keepdims=True) + EPS)
    gated = (jax.nn.sigmoid(ogate) * read * scale * head_gain).astype(jnp.bfloat16)
    local_output = lax.psum(
        jnp.dot(gated, w_out, preferred_element_type=jnp.float32).astype(jnp.bfloat16), "tp"
    ).astype(jnp.float32)
    middle_rows = (tokens.astype(jnp.float32) + local_output).astype(jnp.bfloat16)
    middle = lax.all_to_all(middle_rows, "ep", split_axis=1, concat_axis=0, tiled=True)
    expert_count = w_gate.shape[0] * lax.axis_size("ep")
    topk_count = route.shape[1]
    targets = slot_targets(route, expert_count, EXPERT_CAPACITY)
    buffer = (
        jnp.zeros((expert_count * EXPERT_CAPACITY, col_count), jnp.bfloat16)
        .at[targets]
        .set(jnp.repeat(middle, topk_count, axis=0))
    )
    buffer = buffer.reshape(expert_count, EXPERT_CAPACITY, col_count)
    rows = lax.all_to_all(buffer, "ep", split_axis=0, concat_axis=2, tiled=True)
    rows = norm_rows(rows, ffn_gain)
    gate_v = jnp.einsum("ecd,edf->ecf", rows, w_gate, preferred_element_type=jnp.float32)
    up_v = jnp.einsum("ecd,edf->ecf", rows, w_up, preferred_element_type=jnp.float32)
    activation = (jax.nn.silu(gate_v) * up_v).astype(jnp.bfloat16)
    partial_value = jnp.einsum(
        "ecf,efd->ecd", activation, w_down, preferred_element_type=jnp.float32
    )
    results = lax.psum(partial_value.astype(jnp.bfloat16), "tp")
    returned = lax.all_to_all(results, "ep", split_axis=2, concat_axis=0, tiled=True)
    picked = returned.reshape(expert_count * EXPERT_CAPACITY, col_count)[targets]
    picked = picked.reshape(route.shape[0], topk_count, col_count).astype(jnp.float32)
    weights = route_weight / jnp.sum(route_weight, axis=1, keepdims=True)
    mixed = (middle.astype(jnp.float32) + jnp.sum(picked * weights[:, :, None], axis=1)).astype(
        jnp.bfloat16
    )
    return (mixed, state[:, None], norm_state[:, None], new_max[:, None])


MESH = pl.DeviceIdType.MESH


def dot(a, b):
    return jnp.dot(a, b, preferred_element_type=jnp.float32)


LOAD_ORDER = (
    0,
    1,
    6,
    7,
    8,
    13,
    2,
    3,
    4,
    5,
    12,
    11,
    9,
    10,
    15,
    16,
    14,
    17,
    18,
    19,
)


def layer_kernel(n_ep, n_tp, cap, *refs):
    arguments, refs = refs[: len(LOAD_ORDER)], refs[len(LOAD_ORDER) :]
    (mixed_ref, state_buf, new_normalizer_ref, new_max_ref), refs = refs[:4], refs[4:]
    staged, refs = refs[: len(LOAD_ORDER)], refs[len(LOAD_ORDER) :]
    (
        tokens_ref,
        mix_gain_ref,
        w_query,
        w_key,
        w_value,
        w_ogate,
        w_igate_ref,
        w_fgate_ref,
        forget_bias_ref,
        head_gain_ref,
        w_out,
        memory,
        normalizer_ref,
        running_max_ref,
        ffn_gain_ref,
        route_ref,
        route_weight_ref,
        w_gate,
        w_up,
        w_down,
    ) = staged
    (
        numer_buf,
        tp_rows,
        ep_rows,
        sent_slots,
        ep_slots,
        tp_mixed,
        load_sem,
        tp_send,
        tp_recv,
        ep_send,
        ep_recv,
        slot_send,
        slot_recv,
        mix_send,
        mix_recv,
        round_sem,
    ) = refs
    f32, bf16 = jnp.float32, jnp.bfloat16
    ep, tp = lax.axis_index("ep"), lax.axis_index("tp")
    tp_peers = [
        lax.rem(tp + d, n_tp)
        for d in sorted(range(1, n_tp), key=lambda d: -min(d, n_tp - d))
    ]
    ep_peers = []
    for i in range(n_ep - 1):
        low, high = i, n_ep - 1 - i
        up = jnp.where(high > ep, high, high - 1)
        down = jnp.where(low < ep, low, low + 1)
        ep_peers.append(jnp.where(2 * ep < n_ep, up, down))

    beside = ep + 1 - 2 * lax.rem(ep, 2)
    near = 1 + (ep >= 2).astype(jnp.int32) + (ep < n_ep - 2).astype(jnp.int32)
    rounds = n_ep // 2 - 1

    def greet(sem):
        pl.semaphore_signal(sem, inc=1, device_id={"ep": beside}, device_id_type=MESH)

        @pl.when(ep >= 2)
        def _():
            pl.semaphore_signal(sem, inc=1, device_id={"ep": ep - 2}, device_id_type=MESH)

        @pl.when(ep < n_ep - 2)
        def _():
            pl.semaphore_signal(sem, inc=1, device_id={"ep": ep + 2}, device_id_type=MESH)

    def heard(i):
        if i < rounds:
            pl.semaphore_wait(round_sem.at[i], near)
            if i + 1 < rounds:
                greet(round_sem.at[i + 1])

    barrier = pltpu.get_barrier_semaphore()
    for peer in tp_peers:
        pl.semaphore_signal(barrier, inc=1, device_id={"tp": peer}, device_id_type=MESH)
    greet(barrier)

    loads = {}
    for i in LOAD_ORDER:
        loads[i] = pltpu.make_async_copy(arguments[i], staged[i], load_sem.at[i])
        loads[i].start()

    def arrived(*which):
        for ref in which:
            for i, target in enumerate(staged):
                if target is ref:
                    loads[i].wait()

    def normalized(floats, gain):
        scale = lax.rsqrt(jnp.mean(floats * floats, axis=-1, keepdims=True) + EPS)
        return (floats * scale * gain).astype(bf16)

    own = tokens_ref.shape[0]
    arrived(tokens_ref, mix_gain_ref)
    tokens = tokens_ref[...].astype(f32)
    normed = normalized(tokens, mix_gain_ref[...])
    normed_floats = normed.astype(f32)

    def gate_logit(weight_ref):
        weight = weight_ref[...].astype(f32)
        pick = lax.broadcasted_iota(jnp.int32, weight.shape, 0) == tp
        row = jnp.sum(jnp.where(pick, weight, 0.0), axis=0, keepdims=True)
        return jnp.sum(normed_floats * row, axis=1, keepdims=True)

    arrived(w_igate_ref, w_fgate_ref, forget_bias_ref, running_max_ref)
    log_in = gate_logit(w_igate_ref)
    bias = forget_bias_ref[...]
    bias = jnp.sum(
        jnp.where(lax.broadcasted_iota(jnp.int32, bias.shape, 1) == tp, bias, 0.0),
        axis=1,
        keepdims=True,
    )
    forget_pre = gate_logit(w_fgate_ref) + bias
    log_forget = jnp.minimum(forget_pre, 0.0) - jnp.log1p(jnp.exp(-jnp.abs(forget_pre)))
    eye = lax.broadcasted_iota(jnp.int32, (own, own), 0) == lax.broadcasted_iota(
        jnp.int32, (own, own), 1
    )
    old_max = jnp.sum(jnp.where(eye, running_max_ref[...], 0.0), axis=1, keepdims=True)
    new_max = jnp.maximum(log_forget + old_max, log_in)
    keep = jnp.exp(log_forget + old_max - new_max)
    admit = jnp.exp(log_in - new_max)
    new_max_ref[...] = jnp.sum(jnp.where(eye, new_max, 0.0), axis=0, keepdims=True)

    arrived(w_query)
    query = dot(normed, w_query[...]).astype(bf16).astype(f32)
    arrived(w_key)
    key = dot(normed, w_key[...]).astype(bf16).astype(f32)
    scaled_key = key * w_key.shape[1] ** (-0.5)
    admitted = admit * scaled_key
    arrived(w_value)
    value = dot(normed, w_value[...]).astype(bf16).astype(f32)
    arrived(w_ogate, normalizer_ref)
    ogate = dot(normed, w_ogate[...]).astype(bf16).astype(f32)

    norm_state = keep * normalizer_ref[:, 0, :] + admitted
    new_normalizer_ref[:, 0, :] = norm_state
    denom = jnp.sum(query * norm_state, axis=1, keepdims=True)

    pl.semaphore_wait(barrier, n_tp - 1 + near)
    if rounds:
        greet(round_sem.at[0])

    query_columns = query.T
    key_columns = admitted.T
    arrived(memory)
    for t in range(own):
        state = (
            keep[t : t + 1, :] * memory[t]
            + key_columns[:, t : t + 1] * value[t : t + 1, :]
        )
        state_buf[t] = state
        numer_buf[t : t + 1, :] = jnp.sum(
            query_columns[:, t : t + 1] * state, axis=0, keepdims=True
        )
    arrived(head_gain_ref)
    read = numer_buf[...] / jnp.maximum(jnp.abs(denom), jnp.exp(-new_max))
    scale = lax.rsqrt(jnp.mean(read * read, axis=-1, keepdims=True) + EPS)
    gated = (jax.nn.sigmoid(ogate) * read * scale * head_gain_ref[...]).astype(bf16)
    arrived(w_out)
    tp_rows[tp] = dot(gated, w_out[...]).astype(bf16)

    def exchange(axis, me, peers, source, target, send_sem, recv_sem):
        sends, receipts = [], []
        for peer in peers:
            send = pltpu.make_async_remote_copy(
                src_ref=source(peer),
                dst_ref=target.at[me],
                send_sem=send_sem.at[peer],
                recv_sem=recv_sem.at[me],
                device_id={axis: peer},
                device_id_type=MESH,
            )
            send.start()
            sends.append(send)
            receipts.append(
                pltpu.make_async_remote_copy(
                    src_ref=source(peer),
                    dst_ref=target.at[peer],
                    send_sem=send_sem.at[peer],
                    recv_sem=recv_sem.at[peer],
                    device_id={axis: peer},
                    device_id_type=MESH,
                )
            )
        return sends, receipts

    sends, receipts = exchange(
        "tp", tp, tp_peers, lambda peer: tp_rows.at[tp], tp_rows, tp_send, tp_recv
    )
    all_sends = sends
    heard(0)

    arrived(route_ref, route_weight_ref)
    count = route_ref.shape[1]
    topk = route_ref.shape[0]
    experts = n_ep
    earlier = (
        lax.broadcasted_iota(jnp.int32, (count, count), 0)
        < lax.broadcasted_iota(jnp.int32, (count, count), 1)
    ).astype(bf16)
    weight_rows = route_weight_ref[...]
    weight_rows = weight_rows / jnp.sum(weight_rows, axis=0, keepdims=True)

    def slot_rows(rows, expert):
        named = route_ref[0:1, :] == expert
        for j in range(1, topk):
            named = named | (route_ref[j : j + 1, :] == expert)
        named = named.astype(f32)
        before = dot(named.astype(bf16), earlier)
        slot = lax.broadcasted_iota(jnp.int32, (rows, count), 0) % cap
        return jnp.where(before == slot.astype(f32), named, 0.0)

    mine = slot_rows(cap, jnp.full((cap, count), ep, jnp.int32))
    chosen_weight = jnp.zeros((1, count), f32)
    for j in range(topk):
        chosen_weight = chosen_weight + jnp.where(
            route_ref[j : j + 1, :] == ep, weight_rows[j : j + 1, :], 0.0
        )
    slot_weight = jnp.sum(mine * chosen_weight, axis=1, keepdims=True)
    mine = mine.astype(bf16)
    every = experts * cap
    combine = slot_rows(
        every, lax.broadcasted_iota(jnp.int32, (every, count), 0) // cap
    ).T.astype(bf16)
    heard(1)

    for receipt in receipts:
        receipt.wait_recv()
    summed = tp_rows[0].astype(f32)
    for i in range(1, n_tp):
        summed = summed + tp_rows[i].astype(f32)
    for i in range(2, rounds):
        heard(i)
    ep_rows[ep] = (tokens + summed).astype(bf16)
    sends, receipts = exchange(
        "ep", ep, ep_peers, lambda peer: ep_rows.at[ep], ep_rows, ep_send, ep_recv
    )
    all_sends = all_sends + sends
    arrived(ffn_gain_ref, w_gate, w_up, w_down)
    for receipt in receipts:
        receipt.wait_recv()

    width = tokens.shape[1]
    middle = ep_rows[...].astype(f32).reshape(count, width).astype(bf16)
    rows = normalized(dot(mine, middle), ffn_gain_ref[...])
    gate_v = dot(rows, w_gate[...])
    up_v = dot(rows, w_up[...])
    activation = (gate_v * jax.nn.sigmoid(gate_v) * up_v).astype(bf16)
    partial = (dot(activation, w_down[...]) * slot_weight).astype(bf16)
    columns = width // n_ep
    for c in range(n_ep):
        sent_slots[c] = partial[:, c * columns : (c + 1) * columns]
    sends, receipts = exchange(
        "ep", ep, ep_peers, lambda peer: sent_slots.at[peer], ep_slots, slot_send, slot_recv
    )
    all_sends = all_sends + sends
    ep_slots[ep] = sent_slots[ep]
    own_columns = pl.ds(pl.multiple_of(ep * columns, columns), columns)
    result = ep_rows[:, :, own_columns].astype(f32).reshape(count, columns)
    for receipt in receipts:
        receipt.wait_recv()
    tp_mixed[tp] = dot(combine, ep_slots[...].reshape(every, columns)).astype(bf16)
    sends, receipts = exchange(
        "tp", tp, tp_peers, lambda peer: tp_mixed.at[tp], tp_mixed, mix_send, mix_recv
    )
    all_sends = all_sends + sends
    for receipt in receipts:
        receipt.wait_recv()
    added = tp_mixed[0].astype(f32)
    for i in range(1, n_tp):
        added = added + tp_mixed[i].astype(f32)
    mixed_ref[...] = (result + added).astype(bf16)
    for send in all_sends:
        send.wait_send()


def write_results(*refs):
    sem = refs[-1]
    half = (len(refs) - 1) // 2
    copies = [
        pltpu.make_async_copy(source, target, sem.at[i])
        for i, (source, target) in enumerate(zip(refs[:half], refs[half:-1]))
    ]
    for copy in copies:
        copy.start()
    for copy in copies:
        copy.wait()


def layer(
    tokens,
    mix_gain,
    w_query,
    w_key,
    w_value,
    w_ogate,
    w_igate,
    w_fgate,
    forget_bias,
    head_gain,
    w_out,
    memory,
    normalizer,
    running_max,
    ffn_gain,
    route,
    route_weight,
    w_gate,
    w_up,
    w_down,
):
    n_ep, n_tp = lax.axis_size("ep"), lax.axis_size("tp")
    own, width = tokens.shape
    columns = width // n_ep
    if columns % 128 or own % 8 or n_ep % 2 or w_gate.shape[0] != 1:
        return shards(
            tokens,
            mix_gain,
            w_query,
            w_key,
            w_value,
            w_ogate,
            w_igate,
            w_fgate,
            forget_bias,
            head_gain,
            w_out,
            memory,
            normalizer,
            running_max,
            ffn_gain,
            route,
            route_weight,
            w_gate,
            w_up,
            w_down,
        )
    cap = EXPERT_CAPACITY
    count = route.shape[0]
    anywhere = pl.BlockSpec(memory_space=pltpu.HBM)
    vmem = pl.BlockSpec(memory_space=pltpu.VMEM)
    bf16, f32 = jnp.bfloat16, jnp.float32
    operands = [
        tokens,
        mix_gain[None],
        w_query,
        w_key,
        w_value,
        w_ogate,
        w_igate.T,
        w_fgate.T,
        forget_bias[None],
        head_gain[None],
        w_out,
        memory[:, 0],
        normalizer,
        running_max.T,
        ffn_gain[None],
        route.T,
        route_weight.T,
        w_gate[0],
        w_up[0],
        w_down[0],
    ]
    dma = pltpu.SemaphoreType.DMA
    results = [
        ((count, columns), bf16),
        (memory[:, 0].shape, f32),
        (normalizer.shape, f32),
        ((1, own), f32),
    ]
    held = pl.pallas_call(
        functools.partial(layer_kernel, n_ep, n_tp, cap),
        out_shape=tuple(pltpu.VMEM(*result) for result in results),
        in_specs=[anywhere] * len(operands),
        out_specs=(vmem,) * len(results),
        scratch_shapes=[pltpu.VMEM(a.shape, a.dtype) for a in operands]
        + [
            pltpu.VMEM((own, w_value.shape[1]), f32),
            pltpu.VMEM((n_tp, own, width), bf16),
            pltpu.VMEM((n_ep, own, width), bf16),
            pltpu.VMEM((n_ep, cap, columns), bf16),
            pltpu.VMEM((n_ep, cap, columns), bf16),
            pltpu.VMEM((n_tp, count, columns), bf16),
            dma((len(operands),)),
            dma((n_tp,)),
            dma((n_tp,)),
            dma((n_ep,)),
            dma((n_ep,)),
            dma((n_ep,)),
            dma((n_ep,)),
            dma((n_tp,)),
            dma((n_tp,)),
            pltpu.SemaphoreType.REGULAR((max(1, n_ep // 2 - 1),)),
        ],
        compiler_params=pltpu.CompilerParams(
            collective_id=0, has_side_effects=True
        ),
    )(*operands)
    mixed, new_memory, new_normalizer, new_max = pl.pallas_call(
        write_results,
        out_shape=tuple(jax.ShapeDtypeStruct(*result) for result in results),
        in_specs=[vmem] * len(results),
        out_specs=(anywhere,) * len(results),
        scratch_shapes=[dma((len(results),))],
        compiler_params=pltpu.CompilerParams(vmem_limit_bytes=1024 * 1024),
    )(*held)
    return mixed, new_memory[:, None], new_normalizer, new_max.T


def solution(mesh):
    return jax.shard_map(
        layer,
        mesh=mesh,
        in_specs=(
            P("ep", None),
            P(),
            P(None, "tp"),
            P(None, "tp"),
            P(None, "tp"),
            P(None, "tp"),
            P(),
            P(),
            P(),
            P("tp"),
            P("tp", None),
            P("ep", "tp", None, None),
            P("ep", "tp", None),
            P("ep", "tp"),
            P(),
            P(),
            P(),
            P("ep", None, "tp"),
            P("ep", None, "tp"),
            P("ep", "tp", None),
        ),
        out_specs=(P(None, "ep"), P("ep", "tp", None, None), P("ep", "tp", None), P("ep", "tp")),
        check_vma=False,
    )
```

```python
import functools

import jax
import jax.numpy as jnp
from jax import lax
from jax.experimental import pallas as pl
from jax.experimental.pallas import tpu as pltpu
from jax.sharding import PartitionSpec as P

EXPERT_CAPACITY = 32


EPS = 1e-06


def round_trip(values):
    rounded = lax.optimization_barrier(values.astype(jnp.bfloat16))
    return rounded.astype(jnp.float32)


def norm_rows(values, gain):
    floats = values.astype(jnp.float32)
    scale = lax.rsqrt(jnp.mean(floats * floats, axis=-1, keepdims=True) + EPS)
    return (floats * scale * gain).astype(jnp.bfloat16)


def slot_targets(route, expert_count, capacity):
    flat = route.reshape(-1)
    onehot = (flat[:, None] == jnp.arange(expert_count, dtype=jnp.int32)[None, :]).astype(jnp.int32)
    before = jnp.cumsum(onehot, axis=0) - onehot
    slot = jnp.sum(before * onehot, axis=1)
    return flat * capacity + slot


def shards(
    tokens,
    mix_gain,
    w_query,
    w_key,
    w_value,
    w_ogate,
    w_igate,
    w_fgate,
    forget_bias,
    head_gain,
    w_out,
    memory,
    normalizer,
    running_max,
    ffn_gain,
    route,
    route_weight,
    w_gate,
    w_up,
    w_down,
):
    width = tokens.shape[1]
    col_count = width // lax.axis_size("ep")
    qk_dim = w_query.shape[1]
    normed = norm_rows(tokens, mix_gain)
    query = round_trip(jnp.dot(normed, w_query, preferred_element_type=jnp.float32))
    scaled_key = round_trip(
        jnp.dot(normed, w_key, preferred_element_type=jnp.float32)
    ) * qk_dim ** (-0.5)
    value = round_trip(jnp.dot(normed, w_value, preferred_element_type=jnp.float32))
    ogate = round_trip(jnp.dot(normed, w_ogate, preferred_element_type=jnp.float32))
    head_pick = (jnp.arange(w_igate.shape[1], dtype=jnp.int32) == lax.axis_index("tp")).astype(
        jnp.float32
    )
    log_in = jnp.sum(
        jnp.dot(normed, w_igate, preferred_element_type=jnp.float32) * head_pick, axis=1
    )
    forget_pre = jnp.sum(
        jnp.dot(normed, w_fgate, preferred_element_type=jnp.float32) * head_pick, axis=1
    )
    log_forget = jax.nn.log_sigmoid(forget_pre + jnp.sum(forget_bias * head_pick))
    old_max = running_max[:, 0]
    new_max = jnp.maximum(log_forget + old_max, log_in)
    keep = jnp.exp(log_forget + old_max - new_max)
    admit = jnp.exp(log_in - new_max)
    state = (
        keep[:, None, None] * memory[:, 0]
        + admit[:, None, None] * scaled_key[:, :, None] * value[:, None, :]
    )
    norm_state = keep[:, None] * normalizer[:, 0] + admit[:, None] * scaled_key
    numer = jnp.einsum("tk,tkv->tv", query, state, precision=lax.Precision.HIGHEST)
    denom = jnp.sum(query * norm_state, axis=1)
    read = numer / jnp.maximum(jnp.abs(denom), jnp.exp(-new_max))[:, None]
    scale = lax.rsqrt(jnp.mean(read * read, axis=-1, keepdims=True) + EPS)
    gated = (jax.nn.sigmoid(ogate) * read * scale * head_gain).astype(jnp.bfloat16)
    local_output = lax.psum(
        jnp.dot(gated, w_out, preferred_element_type=jnp.float32).astype(jnp.bfloat16), "tp"
    ).astype(jnp.float32)
    middle_rows = (tokens.astype(jnp.float32) + local_output).astype(jnp.bfloat16)
    middle = lax.all_to_all(middle_rows, "ep", split_axis=1, concat_axis=0, tiled=True)
    expert_count = w_gate.shape[0] * lax.axis_size("ep")
    topk_count = route.shape[1]
    targets = slot_targets(route, expert_count, EXPERT_CAPACITY)
    buffer = (
        jnp.zeros((expert_count * EXPERT_CAPACITY, col_count), jnp.bfloat16)
        .at[targets]
        .set(jnp.repeat(middle, topk_count, axis=0))
    )
    buffer = buffer.reshape(expert_count, EXPERT_CAPACITY, col_count)
    rows = lax.all_to_all(buffer, "ep", split_axis=0, concat_axis=2, tiled=True)
    rows = norm_rows(rows, ffn_gain)
    gate_v = jnp.einsum("ecd,edf->ecf", rows, w_gate, preferred_element_type=jnp.float32)
    up_v = jnp.einsum("ecd,edf->ecf", rows, w_up, preferred_element_type=jnp.float32)
    activation = (jax.nn.silu(gate_v) * up_v).astype(jnp.bfloat16)
    partial_value = jnp.einsum(
        "ecf,efd->ecd", activation, w_down, preferred_element_type=jnp.float32
    )
    results = lax.psum(partial_value.astype(jnp.bfloat16), "tp")
    returned = lax.all_to_all(results, "ep", split_axis=2, concat_axis=0, tiled=True)
    picked = returned.reshape(expert_count * EXPERT_CAPACITY, col_count)[targets]
    picked = picked.reshape(route.shape[0], topk_count, col_count).astype(jnp.float32)
    weights = route_weight / jnp.sum(route_weight, axis=1, keepdims=True)
    mixed = (middle.astype(jnp.float32) + jnp.sum(picked * weights[:, :, None], axis=1)).astype(
        jnp.bfloat16
    )
    return (mixed, state[:, None], norm_state[:, None], new_max[:, None])


MESH = pl.DeviceIdType.MESH


def dot(a, b):
    return jnp.dot(a, b, preferred_element_type=jnp.float32)


LOAD_ORDER = (
    0,
    1,
    6,
    7,
    8,
    13,
    2,
    3,
    4,
    5,
    12,
    11,
    9,
    10,
    15,
    16,
    14,
    17,
    18,
    19,
)


def layer_kernel(n_ep, n_tp, cap, *refs):
    arguments, refs = refs[: len(LOAD_ORDER)], refs[len(LOAD_ORDER) :]
    (mixed_ref, state_buf, new_normalizer_ref, new_max_ref), refs = refs[:4], refs[4:]
    staged, refs = refs[: len(LOAD_ORDER)], refs[len(LOAD_ORDER) :]
    (
        tokens_ref,
        mix_gain_ref,
        w_query,
        w_key,
        w_value,
        w_ogate,
        w_igate_ref,
        w_fgate_ref,
        forget_bias_ref,
        head_gain_ref,
        w_out,
        memory,
        normalizer_ref,
        running_max_ref,
        ffn_gain_ref,
        route_ref,
        route_weight_ref,
        w_gate,
        w_up,
        w_down,
    ) = staged
    (
        numer_buf,
        tp_out,
        tp_rows,
        ep_rows,
        sent_slots,
        ep_slots,
        tp_mixed,
        load_sem,
        tp_send,
        tp_recv,
        ep_send,
        ep_recv,
        pass_send,
        pass_recv,
        slot_send,
        slot_recv,
        mix_send,
        mix_recv,
    ) = refs
    f32, bf16 = jnp.float32, jnp.bfloat16
    ep, tp = lax.axis_index("ep"), lax.axis_index("tp")
    tp_peers = [
        lax.rem(tp + d, n_tp)
        for d in sorted(range(1, n_tp), key=lambda d: -min(d, n_tp - d))
    ]
    ep_peers = []
    for i in range(n_ep - 1):
        low, high = i, n_ep - 1 - i
        up = jnp.where(high > ep, high, high - 1)
        down = jnp.where(low < ep, low, low + 1)
        ep_peers.append(jnp.where(2 * ep < n_ep, up, down))

    barrier = pltpu.get_barrier_semaphore()
    for peer in tp_peers:
        pl.semaphore_signal(barrier, inc=1, device_id={"tp": peer}, device_id_type=MESH)
    for peer in ep_peers:
        pl.semaphore_signal(barrier, inc=1, device_id={"ep": peer}, device_id_type=MESH)

    loads = {}
    for i in LOAD_ORDER:
        loads[i] = pltpu.make_async_copy(arguments[i], staged[i], load_sem.at[i])
        loads[i].start()

    def arrived(*which):
        for ref in which:
            for i, target in enumerate(staged):
                if target is ref:
                    loads[i].wait()

    def normalized(floats, gain):
        scale = lax.rsqrt(jnp.mean(floats * floats, axis=-1, keepdims=True) + EPS)
        return (floats * scale * gain).astype(bf16)

    own = tokens_ref.shape[0]
    arrived(tokens_ref, mix_gain_ref)
    tokens = tokens_ref[...].astype(f32)
    normed = normalized(tokens, mix_gain_ref[...])
    normed_floats = normed.astype(f32)

    def gate_logit(weight_ref):
        weight = weight_ref[...].astype(f32)
        pick = lax.broadcasted_iota(jnp.int32, weight.shape, 0) == tp
        row = jnp.sum(jnp.where(pick, weight, 0.0), axis=0, keepdims=True)
        return jnp.sum(normed_floats * row, axis=1, keepdims=True)

    arrived(w_igate_ref, w_fgate_ref, forget_bias_ref, running_max_ref)
    log_in = gate_logit(w_igate_ref)
    bias = forget_bias_ref[...]
    bias = jnp.sum(
        jnp.where(lax.broadcasted_iota(jnp.int32, bias.shape, 1) == tp, bias, 0.0),
        axis=1,
        keepdims=True,
    )
    forget_pre = gate_logit(w_fgate_ref) + bias
    log_forget = jnp.minimum(forget_pre, 0.0) - jnp.log1p(jnp.exp(-jnp.abs(forget_pre)))
    eye = lax.broadcasted_iota(jnp.int32, (own, own), 0) == lax.broadcasted_iota(
        jnp.int32, (own, own), 1
    )
    old_max = jnp.sum(jnp.where(eye, running_max_ref[...], 0.0), axis=1, keepdims=True)
    new_max = jnp.maximum(log_forget + old_max, log_in)
    keep = jnp.exp(log_forget + old_max - new_max)
    admit = jnp.exp(log_in - new_max)
    new_max_ref[...] = jnp.sum(jnp.where(eye, new_max, 0.0), axis=0, keepdims=True)

    arrived(w_query)
    query = dot(normed, w_query[...]).astype(bf16).astype(f32)
    arrived(w_key)
    key = dot(normed, w_key[...]).astype(bf16).astype(f32)
    scaled_key = key * w_key.shape[1] ** (-0.5)
    admitted = admit * scaled_key
    arrived(w_value)
    value = dot(normed, w_value[...]).astype(bf16).astype(f32)
    arrived(w_ogate, normalizer_ref)
    ogate = dot(normed, w_ogate[...]).astype(bf16).astype(f32)

    norm_state = keep * normalizer_ref[:, 0, :] + admitted
    new_normalizer_ref[:, 0, :] = norm_state
    denom = jnp.sum(query * norm_state, axis=1, keepdims=True)

    query_columns = query.T
    key_columns = admitted.T
    arrived(memory)
    for t in range(own):
        state = (
            keep[t : t + 1, :] * memory[t]
            + key_columns[:, t : t + 1] * value[t : t + 1, :]
        )
        state_buf[t] = state
        numer_buf[t : t + 1, :] = jnp.sum(
            query_columns[:, t : t + 1] * state, axis=0, keepdims=True
        )
    arrived(head_gain_ref)
    read = numer_buf[...] / jnp.maximum(jnp.abs(denom), jnp.exp(-new_max))
    scale = lax.rsqrt(jnp.mean(read * read, axis=-1, keepdims=True) + EPS)
    gated = (jax.nn.sigmoid(ogate) * read * scale * head_gain_ref[...]).astype(bf16)
    arrived(w_out)
    partial = dot(gated, w_out[...]).astype(bf16)
    half_width = partial.shape[1] // 2
    core = lax.rem(tp, 2)
    for h in range(2):
        tp_out[h] = partial[:, h * half_width : (h + 1) * half_width]

    pl.semaphore_wait(barrier, n_tp - 1 + n_ep - 1)

    def exchange(axis, me, peers, source, target, send_sem, recv_sem):
        sends, receipts = [], []
        for peer in peers:
            send = pltpu.make_async_remote_copy(
                src_ref=source(peer),
                dst_ref=target(me),
                send_sem=send_sem.at[peer],
                recv_sem=recv_sem.at[me],
                device_id={axis: peer},
                device_id_type=MESH,
            )
            send.start()
            sends.append(send)
            receipts.append(
                pltpu.make_async_remote_copy(
                    src_ref=source(peer),
                    dst_ref=target(peer),
                    send_sem=send_sem.at[peer],
                    recv_sem=recv_sem.at[peer],
                    device_id={axis: peer},
                    device_id_type=MESH,
                )
            )
        return sends, receipts

    sends, receipts = exchange(
        "tp",
        tp,
        tp_peers,
        lambda peer: tp_out.at[lax.rem(peer, 2)],
        lambda i: tp_rows.at[i],
        tp_send,
        tp_recv,
    )
    tp_rows[tp] = tp_out[core]
    all_sends = sends

    arrived(route_ref, route_weight_ref)
    count = route_ref.shape[1]
    topk = route_ref.shape[0]
    experts = n_ep
    earlier = (
        lax.broadcasted_iota(jnp.int32, (count, count), 0)
        < lax.broadcasted_iota(jnp.int32, (count, count), 1)
    ).astype(bf16)
    weight_rows = route_weight_ref[...]
    weight_rows = weight_rows / jnp.sum(weight_rows, axis=0, keepdims=True)

    def slot_rows(rows, expert):
        named = route_ref[0:1, :] == expert
        for j in range(1, topk):
            named = named | (route_ref[j : j + 1, :] == expert)
        named = named.astype(f32)
        before = dot(named.astype(bf16), earlier)
        slot = lax.broadcasted_iota(jnp.int32, (rows, count), 0) % cap
        return jnp.where(before == slot.astype(f32), named, 0.0)

    mine = slot_rows(cap, jnp.full((cap, count), ep, jnp.int32))
    chosen_weight = jnp.zeros((1, count), f32)
    for j in range(topk):
        chosen_weight = chosen_weight + jnp.where(
            route_ref[j : j + 1, :] == ep, weight_rows[j : j + 1, :], 0.0
        )
    slot_weight = jnp.sum(mine * chosen_weight, axis=1, keepdims=True)
    mine = mine.astype(bf16)
    every = experts * cap
    combine = slot_rows(
        every, lax.broadcasted_iota(jnp.int32, (every, count), 0) // cap
    ).T.astype(bf16)

    for receipt in receipts:
        receipt.wait_recv()
    summed = tp_rows[0].astype(f32)
    for i in range(1, n_tp):
        summed = summed + tp_rows[i].astype(f32)
    own_half = pl.ds(pl.multiple_of(core * half_width, half_width), half_width)
    ep_rows[core, ep] = (tokens_ref[:, own_half].astype(f32) + summed).astype(bf16)
    sends, receipts = exchange(
        "ep",
        ep,
        ep_peers,
        lambda peer: ep_rows.at[core, ep],
        lambda i: ep_rows.at[core, i],
        ep_send,
        ep_recv,
    )
    all_sends = all_sends + sends

    def pass_on(i):
        send = pltpu.make_async_remote_copy(
            src_ref=ep_rows.at[core, i],
            dst_ref=ep_rows.at[core, i],
            send_sem=pass_send.at[i],
            recv_sem=pass_recv.at[i],
            device_id={"tp": tp + 1 - 2 * core},
            device_id_type=MESH,
        )
        send.start()
        return send

    all_sends = all_sends + [pass_on(ep)]
    for peer, receipt in reversed(list(zip(ep_peers, receipts))):
        receipt.wait_recv()
        all_sends = all_sends + [pass_on(peer)]
    arrived(ffn_gain_ref, w_gate, w_up, w_down)
    for i in range(n_ep):
        pltpu.make_async_remote_copy(
            src_ref=ep_rows.at[1 - core, i],
            dst_ref=ep_rows.at[1 - core, i],
            send_sem=pass_send.at[i],
            recv_sem=pass_recv.at[i],
            device_id={"tp": tp + 1 - 2 * core},
            device_id_type=MESH,
        ).wait_recv()

    halves = [
        dot(mine, ep_rows[h].astype(f32).reshape(count, half_width).astype(bf16))
        for h in range(2)
    ]
    width = 2 * half_width
    rows = normalized(jnp.concatenate(halves, axis=1), ffn_gain_ref[...])
    gate_v = dot(rows, w_gate[...])
    up_v = dot(rows, w_up[...])
    activation = (gate_v * jax.nn.sigmoid(gate_v) * up_v).astype(bf16)
    partial = (dot(activation, w_down[...]) * slot_weight).astype(bf16)
    columns = width // n_ep
    for c in range(n_ep):
        sent_slots[c] = partial[:, c * columns : (c + 1) * columns]
    pairs = n_tp // 2
    pair = tp // 2
    receipts = []

    def expert_copy(source, target, to, chip, sem_of, i):
        return pltpu.make_async_remote_copy(
            src_ref=source,
            dst_ref=target,
            send_sem=slot_send.at[chip, to],
            recv_sem=slot_recv.at[sem_of, i],
            device_id={"ep": to, "tp": 2 * chip + core},
            device_id_type=MESH,
        )

    for peer in ep_peers + [ep]:
        for d in reversed(range(pairs)):
            if d or peer is not ep:
                chip = lax.rem(pair + d, pairs)
                send = expert_copy(
                    sent_slots.at[peer], ep_slots.at[pair, ep], peer, chip, pair, ep
                )
                send.start()
                all_sends = all_sends + [send]
                receipts.append(
                    expert_copy(
                        sent_slots.at[peer], ep_slots.at[chip, peer], peer, chip, chip, peer
                    )
                )
    ep_slots[pair, ep] = sent_slots[ep]
    per_half = n_ep // 2
    offset = pl.multiple_of(lax.rem(ep, per_half) * columns, columns)
    result = ep_rows[ep // per_half, :, :, pl.ds(offset, columns)].astype(f32).reshape(count, columns)
    for receipt in receipts:
        receipt.wait_recv()
    gathered = dot(combine, ep_slots[0].reshape(every, columns))
    for i in range(1, pairs):
        gathered = gathered + dot(combine, ep_slots[i].reshape(every, columns))
    tp_mixed[core] = gathered.astype(bf16)
    last = [
        pltpu.make_async_remote_copy(
            src_ref=tp_mixed.at[i],
            dst_ref=tp_mixed.at[i],
            send_sem=mix_send.at[i],
            recv_sem=mix_recv.at[i],
            device_id={"tp": tp + 1 - 2 * core},
            device_id_type=MESH,
        )
        for i in (core, 1 - core)
    ]
    last[0].start()
    last[1].wait_recv()
    added = tp_mixed[0].astype(f32) + tp_mixed[1].astype(f32)
    mixed_ref[...] = (result + added).astype(bf16)
    last[0].wait_send()
    for send in all_sends:
        send.wait_send()


def write_results(*refs):
    sem = refs[-1]
    half = (len(refs) - 1) // 2
    copies = [
        pltpu.make_async_copy(source, target, sem.at[i])
        for i, (source, target) in enumerate(zip(refs[:half], refs[half:-1]))
    ]
    for copy in copies:
        copy.start()
    for copy in copies:
        copy.wait()


def layer(
    tokens,
    mix_gain,
    w_query,
    w_key,
    w_value,
    w_ogate,
    w_igate,
    w_fgate,
    forget_bias,
    head_gain,
    w_out,
    memory,
    normalizer,
    running_max,
    ffn_gain,
    route,
    route_weight,
    w_gate,
    w_up,
    w_down,
):
    n_ep, n_tp = lax.axis_size("ep"), lax.axis_size("tp")
    own, width = tokens.shape
    columns = width // n_ep
    if columns % 128 or own % 8 or n_ep % 2 or n_tp % 2 or w_gate.shape[0] != 1:
        return shards(
            tokens,
            mix_gain,
            w_query,
            w_key,
            w_value,
            w_ogate,
            w_igate,
            w_fgate,
            forget_bias,
            head_gain,
            w_out,
            memory,
            normalizer,
            running_max,
            ffn_gain,
            route,
            route_weight,
            w_gate,
            w_up,
            w_down,
        )
    cap = EXPERT_CAPACITY
    count = route.shape[0]
    anywhere = pl.BlockSpec(memory_space=pltpu.HBM)
    vmem = pl.BlockSpec(memory_space=pltpu.VMEM)
    bf16, f32 = jnp.bfloat16, jnp.float32
    operands = [
        tokens,
        mix_gain[None],
        w_query,
        w_key,
        w_value,
        w_ogate,
        w_igate.T,
        w_fgate.T,
        forget_bias[None],
        head_gain[None],
        w_out,
        memory[:, 0],
        normalizer,
        running_max.T,
        ffn_gain[None],
        route.T,
        route_weight.T,
        w_gate[0],
        w_up[0],
        w_down[0],
    ]
    dma = pltpu.SemaphoreType.DMA
    results = [
        ((count, columns), bf16),
        (memory[:, 0].shape, f32),
        (normalizer.shape, f32),
        ((1, own), f32),
    ]
    held = pl.pallas_call(
        functools.partial(layer_kernel, n_ep, n_tp, cap),
        out_shape=tuple(pltpu.VMEM(*result) for result in results),
        in_specs=[anywhere] * len(operands),
        out_specs=(vmem,) * len(results),
        scratch_shapes=[pltpu.VMEM(a.shape, a.dtype) for a in operands]
        + [
            pltpu.VMEM((own, w_value.shape[1]), f32),
            pltpu.VMEM((2, own, width // 2), bf16),
            pltpu.VMEM((n_tp, own, width // 2), bf16),
            pltpu.VMEM((2, n_ep, own, width // 2), bf16),
            pltpu.VMEM((n_ep, cap, columns), bf16),
            pltpu.VMEM((n_tp // 2, n_ep, cap, columns), bf16),
            pltpu.VMEM((2, count, columns), bf16),
            dma((len(operands),)),
            dma((n_tp,)),
            dma((n_tp,)),
            dma((n_ep,)),
            dma((n_ep,)),
            dma((n_ep,)),
            dma((n_ep,)),
            dma((n_tp // 2, n_ep)),
            dma((n_tp // 2, n_ep)),
            dma((2,)),
            dma((2,)),
        ],
        compiler_params=pltpu.CompilerParams(
            collective_id=0, has_side_effects=True
        ),
    )(*operands)
    mixed, new_memory, new_normalizer, new_max = pl.pallas_call(
        write_results,
        out_shape=tuple(jax.ShapeDtypeStruct(*result) for result in results),
        in_specs=[vmem] * len(results),
        out_specs=(anywhere,) * len(results),
        scratch_shapes=[dma((len(results),))],
        compiler_params=pltpu.CompilerParams(vmem_limit_bytes=1024 * 1024),
    )(*held)
    return mixed, new_memory[:, None], new_normalizer, new_max.T


def solution(mesh):
    return jax.shard_map(
        layer,
        mesh=mesh,
        in_specs=(
            P("ep", None),
            P(),
            P(None, "tp"),
            P(None, "tp"),
            P(None, "tp"),
            P(None, "tp"),
            P(),
            P(),
            P(),
            P("tp"),
            P("tp", None),
            P("ep", "tp", None, None),
            P("ep", "tp", None),
            P("ep", "tp"),
            P(),
            P(),
            P(),
            P("ep", None, "tp"),
            P("ep", None, "tp"),
            P("ep", "tp", None),
        ),
        out_specs=(P(None, "ep"), P("ep", "tp", None, None), P("ep", "tp", None), P("ep", "tp")),
        check_vma=False,
    )
```
